512 devices in a mesh: gr: 2 (over z_hi), fs: 32 (over z_lo, y), tp: 8 (over x, core).
Axes of the slice: x: 4, y: 4, z: 16 (z_hi: 2, z_lo: 8; z = z_hi * 8 + z_lo), core: 2. Of those that a mesh axis runs over, the one named last changes fastest.
Arguments:
- prompt: bfloat16 [8192, 2048], P(('gr', 'tp'), 'fs'), may hold values from -2.5 to 2.5
- gain_pre: float32 [2048], P(('gr', 'fs')), may hold values from 0.1 to 1.9
- gate_pre: float32 [2048, 5632], P(('gr', 'fs'), 'tp'), may hold values from -6 to 6
- up_pre: float32 [2048, 5632], P(('gr', 'fs'), 'tp'), may hold values from -6 to 6
- down_pre: float32 [2048, 5632], P(('gr', 'fs'), 'tp'), may hold values from -16 to 16
- gain_post: float32 [2048], P(('gr', 'fs')), may hold values from 0.1 to 1.9
- gate_post: float32 [2048, 5632], P(('gr', 'fs'), 'tp'), may hold values from -6 to 6
- up_post: float32 [2048, 5632], P(('gr', 'fs'), 'tp'), may hold values from -6 to 6
- down_post: float32 [2048, 5632], P(('gr', 'fs'), 'tp'), may hold values from -16 to 16
Outputs:
- result: bfloat16 [8192, 2048], P(('gr', 'tp'), 'fs')
- gate_first: bfloat16 [5632, 2048], P('fs')
- up_first: bfloat16 [5632, 2048], P('fs')
- down_first: bfloat16 [5632, 2048], P('fs')
- gate_second: bfloat16 [5632, 2048], P('fs')
- up_second: bfloat16 [5632, 2048], P('fs')
- down_second: bfloat16 [5632, 2048], P('fs')
The draws below stay inside these ranges and needn't reach their ends.
All inputs are finite; a program needn't handle non-finite values.
Results may differ from the reference program's by a relative error of at most 0.028.
Values may be sent and summed in bfloat16 or wider, within the bound.
No kernel may reach another device: no remote copies, remote signals or barrier semaphores. Data moves between devices by JAX's collectives and lax.ppermute only.
A program may use at most 64 MiB of HBM per device.

```python
import jax
import jax.numpy as jnp
from jax import lax

D = 2048
FF = 5632
TOKENS = 8192
N_FS = 32


def spiked(entries, key, source, target, parts, factor):
    def block_of(axis_at):
        return (jnp.arange(entries.shape[axis_at]) // (entries.shape[axis_at] // parts)).reshape((-1,) + (1,) * (entries.ndim - 1 - axis_at))

    near = jax.random.permutation(key, parts)[block_of(target)]
    far = (block_of(target) + parts // 2) % parts
    return jnp.where((block_of(source) == near) | (block_of(source) == far), factor * entries, entries)


def block_levels(stream_key, dims, split, smallest, largest):
    factor_of = 1.0
    for axis_at, blocks in split:
        steps = jax.random.uniform(jax.random.fold_in(jax.random.fold_in(stream_key, 6), axis_at), (blocks,), jnp.float32, smallest / len(split), largest / len(split))
        factor_of = factor_of * jnp.repeat(jnp.exp(steps), dims[axis_at] // blocks).reshape((-1,) + (1,) * (len(dims) - 1 - axis_at))
    return factor_of


def gaussian(stream_key, extent, deviation, reach, cuts=(), held_as=jnp.bfloat16):
    array = deviation * jax.random.normal(stream_key, extent, jnp.float32)
    if cuts:
        array = array * block_levels(stream_key, extent, cuts, -0.22, 0.18)
    return jnp.clip(array, -reach, reach).astype(held_as)


def heavy_noise(rng, dims, deviation, reach, cuts, heavy, held_as=jnp.bfloat16):
    entries = deviation * jax.random.normal(rng, dims, jnp.float32)
    if cuts:
        entries = entries * block_levels(rng, dims, cuts, -0.22, 0.18)
    return jnp.clip(spiked(entries, jax.random.fold_in(rng, 3), *heavy), -reach, reach).astype(held_as)


def setup_inputs(seed: int = 0) -> dict:
    keys = jax.random.split(jax.random.key(seed), 10)
    return {
        "prompt": gaussian(keys[0], (TOKENS, D), 0.3, 2.5, ((0, 16), (1, 32))),
        "gain_pre": jnp.clip(1.0 + 0.18 * jax.random.normal(keys[1], (D,), jnp.float32), 0.1, 1.9),
        "gate_pre": gaussian(keys[2], (D, FF), 1.0, 6.0, ((0, 64), (1, 8)), jnp.float32),
        "up_pre": gaussian(keys[3], (D, FF), 1.0, 6.0, ((0, 64), (1, 8)), jnp.float32),
        "down_pre": heavy_noise(keys[4], (D, FF), 1.0, 16.0, ((0, 64), (1, 8)), (1, 0, 64, 4.0), jnp.float32),
        "gain_post": jnp.clip(1.0 + 0.18 * jax.random.normal(keys[5], (D,), jnp.float32), 0.1, 1.9),
        "gate_post": gaussian(keys[6], (D, FF), 1.0, 6.0, ((0, 64), (1, 8)), jnp.float32),
        "up_post": gaussian(keys[7], (D, FF), 1.0, 6.0, ((0, 64), (1, 8)), jnp.float32),
        "down_post": heavy_noise(keys[8], (D, FF), 1.0, 16.0, ((0, 64), (1, 8)), (1, 0, 64, 4.0), jnp.float32),
    }


norm_eps = 1e-06

def fold_gain(gain, matrix):
    return (gain[:, None] * matrix).astype(jnp.bfloat16).T

def half_step(tokens, w_gate, w_up, w_down):
    row_count = tokens.shape[0]
    widened = tokens.astype(jnp.float32)
    row_scale = lax.rsqrt(lax.optimization_barrier(jnp.mean(widened * widened, axis=1)) + norm_eps) * D ** (-0.5)
    gate_sum = jnp.dot(tokens, w_gate.T, preferred_element_type=jnp.float32) * row_scale[:, None]
    up_sum = jnp.dot(tokens, w_up.T, preferred_element_type=jnp.float32) * row_scale[:, None]
    hidden = (jax.nn.silu(gate_sum) * up_sum).astype(jnp.bfloat16)
    group_width = FF // N_FS
    hidden_blocks = jnp.transpose(hidden.reshape(row_count, N_FS, group_width), (1, 0, 2))
    down_blocks = w_down.reshape(N_FS, group_width, D)

    def add_block(running, pair):
        term = jnp.dot(pair[0], pair[1], preferred_element_type=jnp.float32)
        rounded = lax.optimization_barrier(term.astype(jnp.bfloat16))
        return (running + rounded.astype(jnp.float32), None)
    branch, _ = lax.scan(add_block, jnp.zeros((row_count, D), jnp.float32), (hidden_blocks, down_blocks))
    return (widened + 0.5 * FF ** (-0.5) * branch).astype(jnp.bfloat16)

def reference(prompt, gain_pre, gate_pre, up_pre, down_pre, gain_post, gate_post, up_post, down_post):
    gate_first = fold_gain(gain_pre, gate_pre)
    up_first = fold_gain(gain_pre, up_pre)
    down_first = down_pre.astype(jnp.bfloat16).T
    gate_second = fold_gain(gain_post, gate_post)
    up_second = fold_gain(gain_post, up_post)
    down_second = down_post.astype(jnp.bfloat16).T
    middle = half_step(prompt, gate_first, up_first, down_first)
    result = half_step(middle, gate_second, up_second, down_second)
    return (result, gate_first, up_first, down_first, gate_second, up_second, down_second)
```

```python
import jax
import jax.numpy as jnp
from jax import lax
from jax.sharding import Mesh
from jax.sharding import PartitionSpec as P

D = 2048
FF = 5632
NORM_EPS = 1e-06
GR, ZL, Y, X, CORE = 2, 8, 4, 4, 2
AXES = ("gr", "zl", "y", "x", "core")
F32, BF16 = jnp.float32, jnp.bfloat16
BLOCK = FF // (ZL * Y)
ROWS = D // (GR * ZL * Y)
PAD = 72


def swap(blocks, axis):
    return lax.all_to_all(blocks, axis, split_axis=0, concat_axis=0, tiled=True)


def share(block, axis, size):
    return swap(jnp.broadcast_to(block[None], (size, *block.shape)), axis)


def relayout(gain, gate, up, down):
    rounded = jnp.stack(
        [(gain[:, None] * gate).astype(BF16), (gain[:, None] * up).astype(BF16), down.astype(BF16)]
    )
    to_y = rounded.reshape(3, ROWS, Y, BLOCK).transpose(2, 1, 0, 3).reshape(Y, ROWS, 3 * BLOCK)
    from_y = swap(to_y, "y").reshape(Y * ROWS, 3 * BLOCK)
    turned = from_y.T.reshape(X * CORE, 3 * BLOCK // 8, Y * ROWS)
    turned = jnp.pad(turned, ((0, 0), (0, PAD - 3 * BLOCK // 8), (0, 0)))
    spread = swap(swap(turned, ("x", "core")), "zl")
    both = share(spread, "gr", GR)
    wide = share(both, "x", X)
    full = share(wide, "core", CORE)
    full = full.reshape(CORE, X, GR * ZL, PAD, Y * ROWS)[:, :, :, : 3 * BLOCK // 8]
    full = full.transpose(1, 0, 3, 2, 4).reshape(3, BLOCK, D)
    return full[0], full[1], full[2]


def gathered(tokens):
    by_z = share(tokens, "zl", ZL)
    by_y = share(by_z, "y", Y)
    return by_y.transpose(1, 0, 2, 3).reshape(D, tokens.shape[1])


def summed(partial):
    width = partial.shape[1]
    to_y = partial.astype(BF16).reshape(ZL, Y, D // (ZL * Y), width).transpose(1, 0, 2, 3)
    by_y = jnp.sum(swap(to_y, "y").astype(F32), axis=0).astype(BF16)
    return jnp.sum(swap(by_y, "zl").astype(F32), axis=0)


def half_step(tokens, w_gate, w_up, w_down):
    full = gathered(tokens)
    widened = full.astype(F32)
    row_scale = (lax.rsqrt(jnp.mean(widened * widened, axis=0) + NORM_EPS) * D ** (-0.5))[None, :]
    gate = jnp.dot(w_gate, full, preferred_element_type=F32) * row_scale
    up = jnp.dot(w_up, full, preferred_element_type=F32) * row_scale
    hidden = (jax.nn.silu(gate) * up).astype(BF16)
    partial = lax.dot_general(w_down, hidden, (((0,), (0,)), ((), ())), preferred_element_type=F32)
    return (tokens.astype(F32) + 0.5 * FF ** (-0.5) * summed(partial)).astype(BF16)


def local(prompt, gain_pre, gate_pre, up_pre, down_pre, gain_post, gate_post, up_post, down_post):
    first = relayout(gain_pre, gate_pre, up_pre, down_pre)
    second = relayout(gain_post, gate_post, up_post, down_post)
    middle = half_step(prompt.T, *first)
    result = half_step(middle, *second)
    return (result.T, *first, *second)


def solution(mesh):
    fine = Mesh(mesh.devices.reshape(GR, ZL, Y, X, CORE), AXES)
    tokens = P(("gr", "x", "core"), ("zl", "y"))
    gain = P(("gr", "zl", "y"))
    trained = P(("gr", "zl", "y"), ("x", "core"))
    served = P(("zl", "y"), None)
    return jax.shard_map(
        local,
        mesh=fine,
        in_specs=(tokens, gain, trained, trained, trained, gain, trained, trained, trained),
        out_specs=(tokens,) + (served,) * 6,
        check_vma=False,
    )
```

```python
import jax
import jax.numpy as jnp
from jax import lax
from jax.experimental import pallas as pl
from jax.experimental.pallas import tpu as pltpu
from jax.sharding import Mesh
from jax.sharding import PartitionSpec as P

D = 2048
FF = 5632
NORM_EPS = 1e-06
GR, ZQ, B, Y, X, CORE = 2, 4, 2, 4, 4, 2
AXES = ("gr", "zq", "b", "y", "x", "core")
ZL, TP = ZQ * B, X * CORE
F32, BF16 = jnp.float32, jnp.bfloat16
BLOCK = FF // (ZL * Y)
ROWS = D // (GR * ZL * Y)
PART = BLOCK // TP
PADDED = 24
LANES = Y * ROWS
SPANS = GR * ZL
OWN = 2 * PADDED
FEATS = D // (ZL * Y)


def swap(blocks, axis):
    return lax.all_to_all(blocks, axis, split_axis=0, concat_axis=0, tiled=True)


def share(block, axis, size):
    return swap(jnp.broadcast_to(block[None], (size, *block.shape)), axis)


def from_peer(block, axis, size, flip):
    return lax.ppermute(block, axis, [(i, i ^ flip) for i in range(size)])


def spread(layers):
    cols = jnp.stack([jnp.stack(matrices) for matrices in layers])
    n = cols.shape[0] * 3
    to_y = cols.reshape(n, ROWS, Y, BLOCK).transpose(2, 1, 0, 3).reshape(Y, ROWS, n * BLOCK)
    turned = swap(to_y, "y").reshape(LANES, n * BLOCK).T
    parts = turned.reshape(n, TP, PART, LANES).transpose(1, 0, 2, 3)
    parts = jnp.pad(parts, ((0, 0), (0, 0), (0, PADDED - PART), (0, 0))).reshape(TP, n * PADDED, LANES)
    by_zl = swap(parts, ("x", "core"))
    to_z = jnp.broadcast_to(by_zl[None], (GR, *by_zl.shape)).reshape(SPANS, n * PADDED, LANES)
    here = swap(to_z, ("gr", "zq", "b"))
    return [here[:, i * 3 * PADDED : (i + 1) * 3 * PADDED] for i in range(len(layers))]


def widened(piece):
    near = from_peer(piece, "b", B, 1)
    pair = jnp.stack([piece.reshape(SPANS, 3, PADDED, LANES), near.reshape(SPANS, 3, PADDED, LANES)], axis=2)
    pair = pair.reshape(SPANS, 3 * OWN, LANES)
    mine = jnp.stack([pair] + [from_peer(pair, "x", X, k) for k in range(1, X)])
    other = from_peer(mine, "core", CORE, 1)
    return mine, other


def half_kernel(x_ref, mine_ref, other_ref, out_ref, acc_ref, sq_ref):
    width = x_ref.shape[-1]
    pieces = 2 * X

    def rows(span, lo, hi):
        a = mine_ref[:, span, lo:hi, :].reshape(X * (hi - lo), LANES)
        b = other_ref[:, span, lo:hi, :].reshape(X * (hi - lo), LANES)
        return jnp.concatenate([a, b], axis=0)

    def both(zl, lo, hi):
        return jnp.concatenate([rows(2 * zl, lo, hi), rows(2 * zl + 1, lo, hi)], axis=1)

    acc_ref[...] = jnp.zeros_like(acc_ref)
    sq_ref[...] = jnp.zeros_like(sq_ref)

    def inward(zl, _):
        tokens = x_ref[:, zl].reshape(Y * FEATS, width)
        wide = tokens.astype(F32)
        sq_ref[...] += jnp.sum((wide * wide).reshape(Y * FEATS // 8, 8, width), axis=0)
        acc_ref[...] += jnp.dot(both(zl, 0, 2 * OWN), tokens, preferred_element_type=F32)
        return 0

    lax.fori_loop(0, ZL, inward, 0)
    squares = jnp.sum(sq_ref[...], axis=0, keepdims=True)
    scale = lax.rsqrt(squares / D + NORM_EPS) * D ** (-0.5)
    sums = acc_ref[...].reshape(pieces, 2 * OWN, width)
    gate = sums[:, :OWN].reshape(pieces * OWN, width) * scale
    up = sums[:, OWN:].reshape(pieces * OWN, width) * scale
    hidden = (gate / (1.0 + jnp.exp(-gate)) * up).astype(BF16)

    def outward(zl, _):
        part = lax.dot_general(
            both(zl, 2 * OWN, 3 * OWN), hidden, (((0,), (0,)), ((), ())), preferred_element_type=F32
        )
        out_ref[:, zl] = part.astype(BF16).reshape(Y, FEATS, width)
        return 0

    lax.fori_loop(0, ZL, outward, 0)


def half_partial(tokens, mine, other):
    width = tokens.shape[-1]
    vmem = pl.BlockSpec(memory_space=pltpu.VMEM)
    flops = 2 * 3 * 2 * X * OWN * D * width
    return pl.pallas_call(
        half_kernel,
        out_shape=jax.ShapeDtypeStruct(tokens.shape, BF16),
        in_specs=[vmem] * 3,
        out_specs=vmem,
        scratch_shapes=[pltpu.VMEM((2 * X * 2 * OWN, width), F32), pltpu.VMEM((8, width), F32)],
        cost_estimate=pl.CostEstimate(
            flops=flops, bytes_accessed=2 * (2 * tokens.size + 2 * mine.size), transcendentals=0
        ),
        name="half_step",
    )(tokens, mine, other)


def serve_kernel(at_ref, mine_ref, other_ref, gate_ref, up_ref, down_ref, rows_ref):
    x, core = at_ref[0], at_ref[1]
    for m, out_ref in enumerate((gate_ref, up_ref, down_ref)):
        for xs in range(X):
            k = x ^ xs
            a = mine_ref[k, 0, m * OWN : m * OWN + PADDED, :].astype(F32)
            b = other_ref[k, 0, m * OWN : m * OWN + PADDED, :].astype(F32)
            for c in range(CORE):
                at = (xs * CORE + c) * PART
                rows_ref[at : at + PART, :] = jnp.where(core == c, a, b)[:PART]
        out_ref[...] = rows_ref[...].astype(BF16)


def served(mine, other):
    at = jnp.stack([lax.axis_index("x"), lax.axis_index("core")]).astype(jnp.int32)
    piece = pl.BlockSpec((X, 1, 3 * OWN, LANES), lambda j, at: (0, j, 0, 0))
    out = pl.BlockSpec((BLOCK, LANES), lambda j, at: (0, j))
    return pl.pallas_call(
        serve_kernel,
        out_shape=[jax.ShapeDtypeStruct((BLOCK, D), BF16)] * 3,
        grid_spec=pltpu.PrefetchScalarGridSpec(
            num_scalar_prefetch=1,
            grid=(SPANS,),
            in_specs=[piece, piece],
            out_specs=[out] * 3,
            scratch_shapes=[pltpu.VMEM((BLOCK, LANES), F32)],
        ),
        cost_estimate=pl.CostEstimate(flops=10**8, bytes_accessed=2 * (2 * mine.size + 3 * BLOCK * D), transcendentals=0),
        name="serve",
    )(at, mine, other)


def gathered(tokens):
    by_z = share(tokens, "zq", ZQ)
    by_y = share(by_z, "y", Y)
    return by_y.reshape(Y, ZL, FEATS, tokens.shape[-1])


def summed(partial):
    by_y = jnp.sum(swap(partial, "y").astype(F32), axis=0).astype(BF16)
    to_z = by_y.reshape(ZQ, B, *by_y.shape[1:])
    return jnp.sum(swap(to_z, "zq").astype(F32), axis=0)


def half_step(tokens, mine, other):
    total = summed(half_partial(gathered(tokens), mine, other))
    return (tokens.astype(F32) + 0.5 * FF ** (-0.5) * total).astype(BF16)


def local(prompt, gain_pre, gate_pre, up_pre, down_pre, gain_post, gate_post, up_post, down_post):
    first, second = spread(
        [
            ((gain_pre[:, None] * gate_pre).astype(BF16), (gain_pre[:, None] * up_pre).astype(BF16), down_pre.astype(BF16)),
            ((gain_post[:, None] * gate_post).astype(BF16), (gain_post[:, None] * up_post).astype(BF16), down_post.astype(BF16)),
        ]
    )
    half = prompt.shape[0] // B
    tokens = swap(prompt.T.reshape(FEATS, B, half).transpose(1, 0, 2), "b")
    one = widened(first)
    middle = half_step(tokens, *one)
    two = widened(second)
    result = half_step(middle, *two)
    back = swap(result, "b").transpose(1, 0, 2).reshape(FEATS, B * half)
    return (back.T, *served(*one), *served(*two))


def solution(mesh):
    fine = Mesh(mesh.devices.reshape(GR, ZQ, B, Y, X, CORE), AXES)
    tokens = P(("gr", "x", "core"), ("zq", "b", "y"))
    gain = P(("gr", "zq", "b", "y"))
    trained = P(("gr", "zq", "b", "y"), ("x", "core"))
    rows = P(("zq", "b", "y"), None)
    return jax.shard_map(
        local,
        mesh=fine,
        in_specs=(tokens, gain, trained, trained, trained, gain, trained, trained, trained),
        out_specs=(tokens,) + (rows,) * 6,
        check_vma=False,
    )
```

```python
import jax
import jax.numpy as jnp
from jax import lax
from jax.experimental import pallas as pl
from jax.experimental.pallas import tpu as pltpu
from jax.sharding import Mesh
from jax.sharding import PartitionSpec as P

D = 2048
FF = 5632
NORM_EPS = 1e-06
GR, ZQ, B, Y, X, CORE = 2, 4, 2, 4, 4, 2
AXES = ("gr", "zq", "b", "y", "x", "core")
ZL, TP = ZQ * B, X * CORE
F32, BF16 = jnp.float32, jnp.bfloat16
BLOCK = FF // (ZL * Y)
ROWS = D // (GR * ZL * Y)
PART = BLOCK // TP
PADDED = 24
LANES = Y * ROWS
SPANS = GR * ZL
OWN = 2 * PADDED
FEATS = D // (ZL * Y)


def swap(blocks, axis):
    return lax.all_to_all(blocks, axis, split_axis=0, concat_axis=0, tiled=True)


def share(block, axis, size):
    return swap(jnp.broadcast_to(block[None], (size, *block.shape)), axis)


def from_peer(block, axis, size, flip):
    return lax.ppermute(block, axis, [(i, i ^ flip) for i in range(size)])


def after(value, *others):
    return lax.optimization_barrier((value, *others))[0]


def by_block(layers):
    cols = jnp.stack([jnp.stack(matrices) for matrices in layers])
    n = cols.shape[0] * 3
    to_y = cols.reshape(n, ROWS, Y, BLOCK).transpose(2, 1, 0, 3).reshape(Y, ROWS, n * BLOCK)
    turned = swap(to_y, "y").reshape(LANES, n * BLOCK).T
    parts = turned.reshape(n, TP, PART, LANES).transpose(1, 0, 2, 3)
    return jnp.pad(parts, ((0, 0), (0, 0), (0, PADDED - PART), (0, 0))).reshape(TP, n * PADDED, LANES)


def by_span(parts):
    to_z = jnp.broadcast_to(parts[None], (GR, *parts.shape)).reshape(SPANS, *parts.shape[1:])
    return swap(to_z, ("gr", "zq", "b"))


def paired(piece):
    near = from_peer(piece, "b", B, 1)
    pair = jnp.stack([piece.reshape(SPANS, 3, PADDED, LANES), near.reshape(SPANS, 3, PADDED, LANES)], axis=2)
    return pair.reshape(SPANS, 3 * OWN, LANES)


def widened(pair, *beside):
    pieces = [from_peer(pair, "x", X, k) for k in range(1, X)]
    pieces = lax.optimization_barrier((*pieces, *beside))
    mine = jnp.stack([pair, *pieces[: X - 1]])
    other = from_peer(mine, "core", CORE, 1)
    return mine, other, *pieces[X - 1 :]


def half_kernel(at_ref, x_ref, mine_ref, other_ref, out_ref, acc_ref, sq_ref):
    width = x_ref.shape[-1]
    y, zq = at_ref[0], at_ref[1]
    pieces = 2 * X

    def rows(span, lo, hi):
        a = mine_ref[:, span, lo:hi, :].reshape(X * (hi - lo), LANES)
        b = other_ref[:, span, lo:hi, :].reshape(X * (hi - lo), LANES)
        return jnp.concatenate([a, b], axis=0)

    def both(zl, lo, hi):
        return jnp.concatenate([rows(2 * zl, lo, hi), rows(2 * zl + 1, lo, hi)], axis=1)

    acc_ref[...] = jnp.zeros_like(acc_ref)
    sq_ref[...] = jnp.zeros_like(sq_ref)

    def inward(zl, _):
        z, b = (zl // B) ^ zq, zl % B
        tokens = jnp.concatenate([x_ref[y ^ ys, z, b] for ys in range(Y)], axis=0)
        wide = tokens.astype(F32)
        sq_ref[...] += jnp.sum((wide * wide).reshape(Y * FEATS // 8, 8, width), axis=0)
        acc_ref[...] += jnp.dot(both(zl, 0, 2 * OWN), tokens, preferred_element_type=F32)
        return 0

    lax.fori_loop(0, ZL, inward, 0)
    squares = jnp.sum(sq_ref[...], axis=0, keepdims=True)
    scale = lax.rsqrt(squares / D + NORM_EPS) * D ** (-0.5)
    sums = acc_ref[...].reshape(pieces, 2 * OWN, width)
    gate = sums[:, :OWN].reshape(pieces * OWN, width) * scale
    up = sums[:, OWN:].reshape(pieces * OWN, width) * scale
    hidden = (gate / (1.0 + jnp.exp(-gate)) * up).astype(BF16)

    def outward(zl, _):
        part = lax.dot_general(
            both(zl, 2 * OWN, 3 * OWN), hidden, (((0,), (0,)), ((), ())), preferred_element_type=F32
        )
        out_ref[:, zl] = part.astype(BF16).reshape(Y, FEATS, width)
        return 0

    lax.fori_loop(0, ZL, outward, 0)


def half_partial(at, tokens, mine, other):
    width = tokens.shape[-1]
    vmem = pl.BlockSpec(memory_space=pltpu.VMEM)
    flops = 2 * 3 * 2 * X * OWN * D * width
    return pl.pallas_call(
        half_kernel,
        out_shape=jax.ShapeDtypeStruct((Y, ZL, FEATS, width), BF16),
        in_specs=[pl.BlockSpec(memory_space=pltpu.SMEM)] + [vmem] * 3,
        out_specs=vmem,
        scratch_shapes=[pltpu.VMEM((2 * X * 2 * OWN, width), F32), pltpu.VMEM((8, width), F32)],
        cost_estimate=pl.CostEstimate(
            flops=flops, bytes_accessed=2 * (2 * tokens.size + 2 * mine.size), transcendentals=0
        ),
        name="half_step",
    )(at, tokens, mine, other)


def serve_kernel(at_ref, mine_ref, other_ref, gate_ref, up_ref, down_ref, rows_ref):
    x, core = at_ref[0], at_ref[1]
    for m, out_ref in enumerate((gate_ref, up_ref, down_ref)):
        for xs in range(X):
            k = x ^ xs
            a = mine_ref[k, 0, m * OWN : m * OWN + PADDED, :].astype(F32)
            b = other_ref[k, 0, m * OWN : m * OWN + PADDED, :].astype(F32)
            for c in range(CORE):
                at = (xs * CORE + c) * PART
                rows_ref[at : at + PART, :] = jnp.where(core == c, a, b)[:PART]
        out_ref[...] = rows_ref[...].astype(BF16)


def served(mine, other):
    piece = pl.BlockSpec((X, 1, 3 * OWN, LANES), lambda j, at: (0, j, 0, 0))
    out = pl.BlockSpec((BLOCK, LANES), lambda j, at: (0, j))
    return pl.pallas_call(
        serve_kernel,
        out_shape=[jax.ShapeDtypeStruct((BLOCK, D), BF16)] * 3,
        grid_spec=pltpu.PrefetchScalarGridSpec(
            num_scalar_prefetch=1,
            grid=(SPANS,),
            in_specs=[piece, piece],
            out_specs=[out] * 3,
            scratch_shapes=[pltpu.VMEM((BLOCK, LANES), F32)],
        ),
        cost_estimate=pl.CostEstimate(flops=10**8, bytes_accessed=2 * (2 * mine.size + 3 * BLOCK * D), transcendentals=0),
        name="serve",
    )(place("x", "core"), mine, other)


def place(*axes):
    return jnp.stack([lax.axis_index(axis) for axis in axes]).astype(jnp.int32)


def traded(first, second):
    low = lax.axis_index("b") == 0
    keep, send = jnp.where(low, first, second), jnp.where(low, second, first)
    got = from_peer(send, "b", B, 1)
    return jnp.where(low, keep, got), jnp.where(low, got, keep)


def around(block, axis, size):
    return jnp.stack([block] + [from_peer(block, axis, size, k) for k in range(1, size)])


def gathered(tokens):
    return share(share(tokens, "zq", ZQ), "y", Y)


def added(tokens, by_y):
    by_y = jnp.sum(by_y.astype(F32), axis=0).astype(BF16)
    to_z = by_y.reshape(ZQ, B, *by_y.shape[1:])
    total = jnp.sum(swap(to_z, "zq").astype(F32), axis=0)
    return (tokens.astype(F32) + 0.5 * FF ** (-0.5) * total).astype(BF16)


def local(prompt, gain_pre, gate_pre, up_pre, down_pre, gain_post, gate_post, up_post, down_post):
    half = prompt.shape[0] // B
    turned = prompt.T
    parts = by_block(
        [
            ((gain_pre[:, None] * gate_pre).astype(BF16), (gain_pre[:, None] * up_pre).astype(BF16), down_pre.astype(BF16)),
            ((gain_post[:, None] * gate_post).astype(BF16), (gain_post[:, None] * up_post).astype(BF16), down_post.astype(BF16)),
        ]
    )
    tokens = jnp.stack(traded(turned[:, :half], turned[:, half:]))
    parts, tokens = lax.optimization_barrier((parts, tokens))
    to_z = swap(parts, ("x", "core"))
    wide = around(tokens, "zq", ZQ)
    to_z, wide = lax.optimization_barrier((to_z, wide))
    piece = by_span(to_z[:, : 3 * PADDED])
    wide = around(wide, "y", Y)
    piece, wide = lax.optimization_barrier((piece, wide))
    pair = paired(piece)
    next_piece = by_span(after(to_z[:, 3 * PADDED :], pair))
    mine, other, next_piece = widened(pair, next_piece)
    mine, other, wide = lax.optimization_barrier((mine, other, wide))
    partial = half_partial(place("y", "zq"), wide, mine, other)
    partial, mine, other, next_piece = lax.optimization_barrier((partial, mine, other, next_piece))
    first = served(mine, other)
    by_y, *first = lax.optimization_barrier((swap(partial, "y"), *first))
    mine, other = widened(paired(next_piece))
    middle = added(tokens, by_y)

    partial = half_partial(jnp.zeros((2,), jnp.int32), gathered(middle), mine, other)
    partial, mine, other = lax.optimization_barrier((partial, mine, other))
    second = served(mine, other)
    by_y, *second = lax.optimization_barrier((swap(partial, "y"), *second))
    result = added(middle, by_y)
    back = jnp.concatenate(traded(result[0], result[1]), axis=1)
    return (back.T, *first, *second)


def solution(mesh):
    fine = Mesh(mesh.devices.reshape(GR, ZQ, B, Y, X, CORE), AXES)
    tokens = P(("gr", "x", "core"), ("zq", "b", "y"))
    gain = P(("gr", "zq", "b", "y"))
    trained = P(("gr", "zq", "b", "y"), ("x", "core"))
    rows = P(("zq", "b", "y"), None)
    return jax.shard_map(
        local,
        mesh=fine,
        in_specs=(tokens, gain, trained, trained, trained, gain, trained, trained, trained),
        out_specs=(tokens,) + (rows,) * 6,
        check_vma=False,
    )
```

```python
import jax
import jax.numpy as jnp
from jax import lax
from jax.experimental import pallas as pl
from jax.experimental.pallas import tpu as pltpu
from jax.sharding import Mesh
from jax.sharding import PartitionSpec as P

D = 2048
FF = 5632
NORM_EPS = 1e-06
GR, ZQ, B, Y, X, CORE = 2, 4, 2, 4, 4, 2
AXES = ("gr", "zq", "b", "y", "x", "core")
ZL, TP = ZQ * B, X * CORE
F32, BF16 = jnp.float32, jnp.bfloat16
BLOCK = FF // (ZL * Y)
ROWS = D // (GR * ZL * Y)
PART = BLOCK // TP
PADDED = 24
LANES = Y * ROWS
SPANS = GR * ZL
OWN = 2 * PADDED
FEATS = D // (ZL * Y)
AT_ONCE = 4


def swap(blocks, axis):
    return lax.all_to_all(blocks, axis, split_axis=0, concat_axis=0, tiled=True)


def share(block, axis, size):
    return swap(jnp.broadcast_to(block[None], (size, *block.shape)), axis)


def from_peer(block, axis, size, flip):
    return lax.ppermute(block, axis, [(i, i ^ flip) for i in range(size)])


def after(value, *others):
    return lax.optimization_barrier((value, *others))[0]


def by_block(layers):
    cols = jnp.stack([jnp.stack(matrices) for matrices in layers])
    n = cols.shape[0] * 3
    to_y = cols.reshape(n, ROWS, Y, BLOCK).transpose(2, 1, 0, 3).reshape(Y, ROWS, n * BLOCK)
    turned = swap(to_y, "y").reshape(LANES, n * BLOCK).T
    parts = turned.reshape(n, TP, PART, LANES).transpose(1, 0, 2, 3)
    return jnp.pad(parts, ((0, 0), (0, 0), (0, PADDED - PART), (0, 0))).reshape(TP, n * PADDED, LANES)


def by_span(parts):
    to_z = jnp.broadcast_to(parts[None], (GR, *parts.shape)).reshape(SPANS, *parts.shape[1:])
    return swap(to_z, ("gr", "zq", "b"))


def paired(piece):
    near = from_peer(piece, "b", B, 1)
    both = jnp.stack([piece.reshape(SPANS, -1, PADDED, LANES), near.reshape(SPANS, -1, PADDED, LANES)], axis=2)
    return [both[:, i : i + 3].reshape(SPANS, 3 * OWN, LANES) for i in range(0, both.shape[1], 3)]


def widened(pair, *beside):
    pieces = [from_peer(pair, "x", X, k) for k in range(1, X)]
    pieces = lax.optimization_barrier((*pieces, *beside))
    mine = jnp.stack([pair, *pieces[: X - 1]])
    other = from_peer(mine, "core", CORE, 1)
    return mine, other, *pieces[X - 1 :]


def half_kernel(x_ref, mine_ref, other_ref, out_ref, acc_ref, sq_ref):
    width = x_ref.shape[-1]
    pieces = 2 * X

    def rows(span, lo, hi):
        a = mine_ref[:, span, lo:hi, :].reshape(X * (hi - lo), LANES)
        b = other_ref[:, span, lo:hi, :].reshape(X * (hi - lo), LANES)
        return jnp.concatenate([a, b], axis=0)

    def both(zl, lo, hi):
        return jnp.concatenate([rows(2 * zl, lo, hi), rows(2 * zl + 1, lo, hi)], axis=1)

    acc_ref[...] = jnp.zeros_like(acc_ref)
    sq_ref[...] = jnp.zeros_like(sq_ref)

    def inward(zl, _):
        tokens = x_ref[:, zl].reshape(Y * FEATS, width)
        wide = tokens.astype(F32)
        sq_ref[...] += jnp.sum((wide * wide).reshape(Y * FEATS // 8, 8, width), axis=0)
        acc_ref[...] += jnp.dot(both(zl, 0, 2 * OWN), tokens, preferred_element_type=F32)
        return 0

    lax.fori_loop(0, ZL, inward, 0)
    squares = jnp.sum(sq_ref[...], axis=0, keepdims=True)
    scale = lax.rsqrt(squares / D + NORM_EPS) * D ** (-0.5)
    sums = acc_ref[...].reshape(pieces, 2 * OWN, width)
    gate = sums[:, :OWN].reshape(pieces * OWN, width) * scale
    up = sums[:, OWN:].reshape(pieces * OWN, width) * scale
    hidden = (gate / (1.0 + jnp.exp(-gate)) * up).astype(BF16)

    def outward(zl, _):
        part = lax.dot_general(
            both(zl, 2 * OWN, 3 * OWN), hidden, (((0,), (0,)), ((), ())), preferred_element_type=F32
        )
        out_ref[:, zl] = part.astype(BF16).reshape(Y, FEATS, width)
        return 0

    lax.fori_loop(0, ZL, outward, 0)


def half_partial(tokens, mine, other):
    width = tokens.shape[-1]
    vmem = pl.BlockSpec(memory_space=pltpu.VMEM)
    flops = 2 * 3 * 2 * X * OWN * D * width
    return pl.pallas_call(
        half_kernel,
        out_shape=jax.ShapeDtypeStruct((Y, ZL, FEATS, width), BF16),
        in_specs=[vmem] * 3,
        out_specs=vmem,
        scratch_shapes=[pltpu.VMEM((2 * X * 2 * OWN, width), F32), pltpu.VMEM((8, width), F32)],
        cost_estimate=pl.CostEstimate(
            flops=flops, bytes_accessed=2 * (2 * tokens.size + 2 * mine.size), transcendentals=0
        ),
        name="half_step",
    )(tokens, mine, other)


def serve_kernel(at_ref, mine_ref, other_ref, gate_ref, up_ref, down_ref, rows_ref):
    x, core = at_ref[0], at_ref[1]
    for span in range(AT_ONCE):
        for m, out_ref in enumerate((gate_ref, up_ref, down_ref)):
            for xs in range(X):
                k = x ^ xs
                a = mine_ref[k, span, m * OWN : m * OWN + PADDED, :].astype(F32)
                b = other_ref[k, span, m * OWN : m * OWN + PADDED, :].astype(F32)
                for c in range(CORE):
                    at = (xs * CORE + c) * PART
                    rows_ref[m, at : at + PART, :] = jnp.where(core == c, a, b)[:PART]
            out_ref[:, span * LANES : (span + 1) * LANES] = rows_ref[m].astype(BF16)


def served(mine, other):
    piece = pl.BlockSpec((X, AT_ONCE, 3 * OWN, LANES), lambda j, at: (0, j, 0, 0))
    out = pl.BlockSpec((BLOCK, AT_ONCE * LANES), lambda j, at: (0, j))
    return pl.pallas_call(
        serve_kernel,
        out_shape=[jax.ShapeDtypeStruct((BLOCK, D), BF16)] * 3,
        grid_spec=pltpu.PrefetchScalarGridSpec(
            num_scalar_prefetch=1,
            grid=(SPANS // AT_ONCE,),
            in_specs=[piece, piece],
            out_specs=[out] * 3,
            scratch_shapes=[pltpu.VMEM((3, BLOCK, LANES), F32)],
        ),
        cost_estimate=pl.CostEstimate(flops=10**8, bytes_accessed=2 * (2 * mine.size + 3 * BLOCK * D), transcendentals=0),
        name="serve",
    )(place("x", "core"), mine, other)


def place(*axes):
    return jnp.stack([lax.axis_index(axis) for axis in axes]).astype(jnp.int32)


def traded(first, second):
    low = lax.axis_index("b") == 0
    keep, send = jnp.where(low, first, second), jnp.where(low, second, first)
    got = from_peer(send, "b", B, 1)
    return jnp.where(low, keep, got), jnp.where(low, got, keep)


def gathered(tokens):
    return share(share(tokens, "zq", ZQ), "y", Y).reshape(Y, ZL, FEATS, tokens.shape[-1])


def over_y(blocks):
    return jnp.sum(blocks.astype(F32), axis=0).astype(BF16)


def stepped(tokens, total):
    return (tokens.astype(F32) + 0.5 * FF ** (-0.5) * total).astype(BF16)


def local(prompt, gain_pre, gate_pre, up_pre, down_pre, gain_post, gate_post, up_post, down_post):
    half = prompt.shape[0] // B
    turned = prompt.T
    parts = by_block(
        [
            ((gain_pre[:, None] * gate_pre).astype(BF16), (gain_pre[:, None] * up_pre).astype(BF16), down_pre.astype(BF16)),
            ((gain_post[:, None] * gate_post).astype(BF16), (gain_post[:, None] * up_post).astype(BF16), down_post.astype(BF16)),
        ]
    )
    piece = by_span(swap(parts, ("x", "core")))
    one, two = paired(piece)
    tokens = jnp.stack(traded(turned[:, :half], turned[:, half:]))
    wide = gathered(after(tokens, one))
    mine, other, wide = widened(one, wide)
    partial = half_partial(wide, mine, other)
    partial, mine, other, two = lax.optimization_barrier((partial, mine, other, two))
    first = served(mine, other)
    mine, other = widened(two)
    sums = over_y(swap(partial, "y"))
    sums = swap(sums.reshape(ZQ, B, *sums.shape[1:]), "zq")
    sums, *first = lax.optimization_barrier((sums, *first))
    middle = stepped(tokens, jnp.sum(sums.astype(F32), axis=0))

    partial = half_partial(gathered(middle), mine, other)
    partial, mine, other = lax.optimization_barrier((partial, mine, other))
    second = served(mine, other)
    by_y, *second = lax.optimization_barrier((swap(partial, "y"), *second))
    sums = swap(over_y(by_y), ("zq", "b")).reshape(ZQ, B, FEATS, half)
    total = jnp.sum(sums.astype(F32), axis=0)
    own = jnp.stack(traded(middle[0], middle[1]))
    result = stepped(own, total)
    back = result.transpose(1, 0, 2).reshape(FEATS, B * half)
    return (back.T, *first, *second)


def solution(mesh):
    fine = Mesh(mesh.devices.reshape(GR, ZQ, B, Y, X, CORE), AXES)
    tokens = P(("gr", "x", "core"), ("zq", "b", "y"))
    gain = P(("gr", "zq", "b", "y"))
    trained = P(("gr", "zq", "b", "y"), ("x", "core"))
    rows = P(("zq", "b", "y"), None)
    return jax.shard_map(
        local,
        mesh=fine,
        in_specs=(tokens, gain, trained, trained, trained, gain, trained, trained, trained),
        out_specs=(tokens,) + (rows,) * 6,
        check_vma=False,
    )
```

```python
import jax
import jax.numpy as jnp
from jax import lax
from jax.experimental import pallas as pl
from jax.experimental.pallas import tpu as pltpu
from jax.sharding import Mesh
from jax.sharding import PartitionSpec as P

D = 2048
FF = 5632
NORM_EPS = 1e-06
GR, ZQ, B, Y, X, CORE = 2, 4, 2, 4, 4, 2
AXES = ("gr", "zq", "b", "y", "x", "core")
ZL, TP = ZQ * B, X * CORE
F32, BF16 = jnp.float32, jnp.bfloat16
BLOCK = FF // (ZL * Y)
ROWS = D // (GR * ZL * Y)
PART = BLOCK // TP
PADDED = 24
LANES = Y * ROWS
SPANS = GR * ZL
OWN = 2 * PADDED
FEATS = D // (ZL * Y)
AT_ONCE = 4


def swap(blocks, axis):
    return lax.all_to_all(blocks, axis, split_axis=0, concat_axis=0, tiled=True)


def share(block, axis, size):
    return swap(jnp.broadcast_to(block[None], (size, *block.shape)), axis)


def from_peer(block, axis, size, flip):
    return lax.ppermute(block, axis, [(i, i ^ flip) for i in range(size)])


def after(value, *others):
    return lax.optimization_barrier((value, *others))[0]


def by_block(layers):
    cols = jnp.stack([jnp.stack(matrices) for matrices in layers])
    n = cols.shape[0] * 3
    to_y = cols.reshape(n, ROWS, Y, BLOCK).transpose(2, 1, 0, 3).reshape(Y, ROWS, n * BLOCK)
    turned = swap(to_y, "y").reshape(LANES, n * BLOCK).T
    parts = turned.reshape(n, TP, PART, LANES).transpose(1, 0, 2, 3)
    return jnp.pad(parts, ((0, 0), (0, 0), (0, PADDED - PART), (0, 0))).reshape(TP, n * PADDED, LANES)


def by_span(parts):
    to_z = jnp.broadcast_to(parts.reshape(1, ZQ, -1, LANES), (GR, ZQ, B * parts.shape[1], LANES))
    here = swap(to_z.reshape(GR * ZQ, B * parts.shape[1], LANES), ("gr", "zq"))
    here = here.reshape(GR * ZQ, B, -1, 3, PADDED, LANES).transpose(2, 0, 3, 1, 4, 5)
    return here.reshape(-1, GR * ZQ, 3 * OWN, LANES)


def paired(piece):
    near = from_peer(piece, "b", B, 1)
    low = lax.axis_index("b") == 0
    both = jnp.stack([jnp.where(low, piece, near), jnp.where(low, near, piece)], axis=1)
    return both.reshape(SPANS, 3 * OWN, LANES)


def over_x(pair):
    return [from_peer(pair, "x", X, k) for k in range(1, X)]


def widened(pair, pieces):
    mine = jnp.stack([pair, *pieces])
    return mine, from_peer(mine, "core", CORE, 1)


def slot(zl, zq):
    k = (zl // B) ^ zq
    return ((k & 1) << 1) | (k >> 1), zl % B


def half_kernel(at_ref, x_ref, mine_ref, other_ref, out_ref, acc_ref, sq_ref):
    width = x_ref.shape[-1]
    pieces = 2 * X
    zq = at_ref[0]

    def rows(span, lo, hi):
        a = mine_ref[:, span, lo:hi, :].reshape(X * (hi - lo), LANES)
        b = other_ref[:, span, lo:hi, :].reshape(X * (hi - lo), LANES)
        return jnp.concatenate([a, b], axis=0)

    def both(zl, lo, hi):
        return jnp.concatenate([rows(2 * zl, lo, hi), rows(2 * zl + 1, lo, hi)], axis=1)

    acc_ref[...] = jnp.zeros_like(acc_ref)
    sq_ref[...] = jnp.zeros_like(sq_ref)

    def inward(zl, _):
        k, b = slot(zl, zq)
        tokens = x_ref[:, k, b].reshape(Y * FEATS, width)
        wide = tokens.astype(F32)
        sq_ref[...] += jnp.sum((wide * wide).reshape(Y * FEATS // 8, 8, width), axis=0)
        acc_ref[...] += jnp.dot(both(zl, 0, 2 * OWN), tokens, preferred_element_type=F32)
        return 0

    lax.fori_loop(0, ZL, inward, 0)
    squares = jnp.sum(sq_ref[...], axis=0, keepdims=True)
    scale = lax.rsqrt(squares / D + NORM_EPS) * D ** (-0.5)
    sums = acc_ref[...].reshape(pieces, 2 * OWN, width)
    gate = sums[:, :OWN].reshape(pieces * OWN, width) * scale
    up = sums[:, OWN:].reshape(pieces * OWN, width) * scale
    hidden = (gate / (1.0 + jnp.exp(-gate)) * up).astype(BF16)

    def outward(zl, _):
        part = lax.dot_general(
            both(zl, 2 * OWN, 3 * OWN), hidden, (((0,), (0,)), ((), ())), preferred_element_type=F32
        )
        k, b = slot(zl, zq)
        out_ref[:, k, b] = part.astype(BF16).reshape(Y, FEATS, width)
        return 0

    lax.fori_loop(0, ZL, outward, 0)


def half_partial(tokens, mine, other):
    width = tokens.shape[-1]
    vmem = pl.BlockSpec(memory_space=pltpu.VMEM)
    flops = 2 * 3 * 2 * X * OWN * D * width
    return pl.pallas_call(
        half_kernel,
        out_shape=jax.ShapeDtypeStruct(tokens.shape, BF16),
        in_specs=[pl.BlockSpec(memory_space=pltpu.SMEM)] + [vmem] * 3,
        out_specs=vmem,
        scratch_shapes=[pltpu.VMEM((2 * X * 2 * OWN, width), F32), pltpu.VMEM((8, width), F32)],
        cost_estimate=pl.CostEstimate(
            flops=flops, bytes_accessed=2 * (2 * tokens.size + 2 * mine.size), transcendentals=0
        ),
        name="half_step",
    )(place("zq"), tokens, mine, other)


def serve_kernel(at_ref, mine_ref, other_ref, gate_ref, up_ref, down_ref, rows_ref):
    x, core, b = at_ref[0], at_ref[1], at_ref[2]
    for span in range(AT_ONCE):
        for m, out_ref in enumerate((gate_ref, up_ref, down_ref)):
            for xs in range(X):
                k = x ^ xs
                own = pl.ds(pl.multiple_of(m * OWN + b * PADDED, 8), PADDED)
                north = mine_ref[k, span, own, :].astype(F32)
                south = other_ref[k, span, own, :].astype(F32)
                for c in range(CORE):
                    at = (xs * CORE + c) * PART
                    rows_ref[m, at : at + PART, :] = jnp.where(core == c, north, south)[:PART]
            out_ref[:, span * LANES : (span + 1) * LANES] = rows_ref[m].astype(BF16)


def served(mine, other):
    piece = pl.BlockSpec((X, AT_ONCE, 3 * OWN, LANES), lambda j, at: (0, j, 0, 0))
    out = pl.BlockSpec((BLOCK, AT_ONCE * LANES), lambda j, at: (0, j))
    return pl.pallas_call(
        serve_kernel,
        out_shape=[jax.ShapeDtypeStruct((BLOCK, D), BF16)] * 3,
        grid_spec=pltpu.PrefetchScalarGridSpec(
            num_scalar_prefetch=1,
            grid=(SPANS // AT_ONCE,),
            in_specs=[piece, piece],
            out_specs=[out] * 3,
            scratch_shapes=[pltpu.VMEM((3, BLOCK, LANES), F32)],
        ),
        cost_estimate=pl.CostEstimate(flops=10**8, bytes_accessed=2 * (2 * mine.size + 3 * BLOCK * D), transcendentals=0),
        name="serve",
    )(place("x", "core", "b"), mine, other)


def place(*axes):
    return jnp.stack([lax.axis_index(axis) for axis in axes]).astype(jnp.int32)


def traded(first, second):
    low = lax.axis_index("b") == 0
    keep, send = jnp.where(low, first, second), jnp.where(low, second, first)
    got = from_peer(send, "b", B, 1)
    return jnp.where(low, keep, got), jnp.where(low, got, keep)


def over_zq(tokens):
    two = jnp.stack([tokens, from_peer(tokens, "zq", ZQ, 2)])
    return jnp.concatenate([two, from_peer(two, "zq", ZQ, 1)])


def summed(by_y):
    send = jnp.sum(by_y[:, ZQ // 2 :].astype(F32), axis=0).astype(BF16)
    got = from_peer(send, "zq", ZQ, 1)
    kept = jnp.sum(by_y[:, : ZQ // 2].astype(F32), axis=0) + got.astype(F32)
    return kept[0] + from_peer(kept[1].astype(BF16), "zq", ZQ, 2).astype(F32)


def stepped(tokens, total):
    return (tokens.astype(F32) + 0.5 * FF ** (-0.5) * total).astype(BF16)


def local(prompt, gain_pre, gate_pre, up_pre, down_pre, gain_post, gate_post, up_post, down_post):
    half = prompt.shape[0] // B
    turned = prompt.T
    parts = by_block(
        [
            ((gain_pre[:, None] * gate_pre).astype(BF16), (gain_pre[:, None] * up_pre).astype(BF16), down_pre.astype(BF16)),
            ((gain_post[:, None] * gate_post).astype(BF16), (gain_post[:, None] * up_post).astype(BF16), down_post.astype(BF16)),
        ]
    )
    to_z = swap(parts, ("x", "core"))
    tokens = jnp.stack(traded(turned[:, :half], turned[:, half:]))
    wide = over_zq(after(tokens, to_z))
    one, two = by_span(to_z)
    one, two, wide = lax.optimization_barrier((one, two, wide))
    one = paired(one)
    pieces = over_x(one)
    two = paired(after(two, one))
    wide = share(after(wide, one), "y", Y)
    *pieces, two, wide = lax.optimization_barrier((*pieces, two, wide))
    mine, other = widened(one, pieces)
    partial = half_partial(wide, mine, other)
    partial, mine, other, two = lax.optimization_barrier((partial, mine, other, two))
    first = served(mine, other)
    pieces = over_x(two)
    by_y = swap(partial, "y")
    total, *first = lax.optimization_barrier((summed(by_y), *first))
    *pieces, total = lax.optimization_barrier((*pieces, total))
    mine, other = widened(two, pieces)
    middle = stepped(tokens, total)

    partial = half_partial(share(over_zq(middle), "y", Y), mine, other)
    partial, mine, other = lax.optimization_barrier((partial, mine, other))
    second = served(mine, other)
    by_y, *second = lax.optimization_barrier((swap(partial, "y"), *second))
    result = stepped(middle, summed(by_y))
    back = jnp.concatenate(traded(result[0], result[1]), axis=1)
    return (back.T, *first, *second)


def solution(mesh):
    fine = Mesh(mesh.devices.reshape(GR, ZQ, B, Y, X, CORE), AXES)
    tokens = P(("gr", "x", "core"), ("zq", "b", "y"))
    gain = P(("gr", "zq", "b", "y"))
    trained = P(("gr", "zq", "b", "y"), ("x", "core"))
    rows = P(("zq", "b", "y"), None)
    return jax.shard_map(
        local,
        mesh=fine,
        in_specs=(tokens, gain, trained, trained, trained, gain, trained, trained, trained),
        out_specs=(tokens,) + (rows,) * 6,
        check_vma=False,
    )
```

```python
import jax
import jax.numpy as jnp
from jax import lax
from jax.experimental import pallas as pl
from jax.experimental.pallas import tpu as pltpu
from jax.sharding import Mesh
from jax.sharding import PartitionSpec as P

D = 2048
FF = 5632
NORM_EPS = 1e-06
GR, ZQ, B, Y, X, CORE = 2, 4, 2, 4, 4, 2
AXES = ("gr", "zq", "b", "y", "x", "core")
ZL = ZQ * B
F32, BF16 = jnp.float32, jnp.bfloat16
BLOCK = FF // (ZL * Y)
ROWS = D // (GR * ZL * Y)
PART = BLOCK // X
PADDED = 48
LANES = Y * ROWS
SPANS = GR * ZL
PIECE = 3 * PADDED
FEATS = D // (ZL * Y)
AT_ONCE = 4


def swap(blocks, axis):
    return lax.all_to_all(blocks, axis, split_axis=0, concat_axis=0, tiled=True)


def share(block, axis, size):
    return swap(jnp.broadcast_to(block[None], (size, *block.shape)), axis)


def from_peer(block, axis, size, flip):
    return lax.ppermute(block, axis, [(i, i ^ flip) for i in range(size)])


def after(value, *others):
    return lax.optimization_barrier((value, *others))[0]


def by_block(layers):
    cols = jnp.stack([matrix for matrices in layers for matrix in matrices])
    n = cols.shape[0]
    to_yx = cols.reshape(n, ROWS, Y * X, PART).transpose(2, 1, 0, 3).reshape(Y * X, ROWS, n * PART)
    here = swap(to_yx, ("y", "x")).reshape(Y, X, ROWS, n * PART)
    turned = here.transpose(1, 3, 0, 2).reshape(X, n, PART, LANES)
    return jnp.pad(turned, ((0, 0), (0, 0), (0, PADDED - PART), (0, 0))).reshape(X, n * PADDED, LANES)


def by_span(parts):
    to_z = jnp.broadcast_to(parts[None], (GR, *parts.shape)).reshape(GR * ZQ, *parts.shape[1:])
    here = swap(to_z, ("gr", "zq"))
    return [here[:, i : i + PIECE] for i in range(0, here.shape[1], PIECE)]


def paired(piece):
    near = from_peer(piece, "b", B, 1)
    low = lax.axis_index("b") == 0
    both = jnp.stack([jnp.where(low, piece, near), jnp.where(low, near, piece)], axis=1)
    return both.reshape(SPANS, PIECE, LANES)


def over_x(pair):
    return [pair] + [from_peer(pair, "x", X, k) for k in range(1, X)]


def over_core(pieces):
    return [from_peer(piece, "core", CORE, 1) for piece in pieces]


def slot(zl, zq):
    k = (zl // B) ^ zq
    return ((k & 1) << 1) | (k >> 1), zl % B


def half_kernel(at_ref, x_ref, *refs):
    piece_refs, (out_ref, acc_ref, sq_ref) = refs[: 2 * X], refs[2 * X :]
    width = x_ref.shape[-1]
    pieces = 2 * X
    zq = at_ref[0]

    def rows(span, lo, hi):
        return jnp.concatenate([ref[span, lo:hi, :] for ref in piece_refs], axis=0)

    def both(zl, lo, hi):
        return jnp.concatenate([rows(2 * zl, lo, hi), rows(2 * zl + 1, lo, hi)], axis=1)

    acc_ref[...] = jnp.zeros_like(acc_ref)
    sq_ref[...] = jnp.zeros_like(sq_ref)

    def inward(zl, _):
        k, b = slot(zl, zq)
        tokens = x_ref[:, k, b].reshape(Y * FEATS, width)
        wide = tokens.astype(F32)
        sq_ref[...] += jnp.sum((wide * wide).reshape(Y * FEATS // 8, 8, width), axis=0)
        acc_ref[...] += jnp.dot(both(zl, 0, 2 * PADDED), tokens, preferred_element_type=F32)
        return 0

    lax.fori_loop(0, ZL, inward, 0)
    squares = jnp.sum(sq_ref[...], axis=0, keepdims=True)
    scale = lax.rsqrt(squares / D + NORM_EPS) * D ** (-0.5)
    sums = acc_ref[...].reshape(pieces, 2 * PADDED, width)
    gate = sums[:, :PADDED].reshape(pieces * PADDED, width) * scale
    up = sums[:, PADDED:].reshape(pieces * PADDED, width) * scale
    hidden = (gate / (1.0 + jnp.exp(-gate)) * up).astype(BF16)

    def outward(zl, _):
        part = lax.dot_general(
            both(zl, 2 * PADDED, PIECE), hidden, (((0,), (0,)), ((), ())), preferred_element_type=F32
        )
        k, b = slot(zl, zq)
        out_ref[:, k, b] = part.astype(BF16).reshape(Y, FEATS, width)
        return 0

    lax.fori_loop(0, ZL, outward, 0)


def half_partial(tokens, pieces):
    width = tokens.shape[-1]
    vmem = pl.BlockSpec(memory_space=pltpu.VMEM)
    flops = 2 * 3 * 2 * X * PADDED * D * width
    return pl.pallas_call(
        half_kernel,
        out_shape=jax.ShapeDtypeStruct(tokens.shape, BF16),
        in_specs=[pl.BlockSpec(memory_space=pltpu.SMEM)] + [vmem] * (1 + 2 * X),
        out_specs=vmem,
        scratch_shapes=[pltpu.VMEM((2 * X * 2 * PADDED, width), F32), pltpu.VMEM((8, width), F32)],
        cost_estimate=pl.CostEstimate(
            flops=flops, bytes_accessed=2 * (2 * tokens.size + 2 * X * pieces[0].size), transcendentals=0
        ),
        name="half_step",
    )(place("zq"), tokens, *pieces)


def serve_kernel(at_ref, *refs):
    piece_refs, out_refs, rows_ref = refs[: 2 * X], refs[2 * X : -1], refs[-1]
    x, here = at_ref[0], at_ref[1] == at_ref[2]
    odd, high = (x & 1) == 1, (x & 2) == 2
    for span in range(AT_ONCE):
        for m, out_ref in enumerate(out_refs):
            lo, hi = m * PADDED, (m + 1) * PADDED
            mine = [ref[span, lo:hi, :].astype(F32) for ref in piece_refs[:X]]
            other = [ref[span, lo:hi, :].astype(F32) for ref in piece_refs[X:]]
            p = [jnp.where(here, a, b) for a, b in zip(mine, other)]
            p = [jnp.where(odd, p[k ^ 1], p[k]) for k in range(X)]
            p = [jnp.where(high, p[k ^ 2], p[k]) for k in range(X)]
            for k in range(X):
                rows_ref[m, k * PART : (k + 1) * PART, :] = p[k][:PART]
            out_ref[:, span * LANES : (span + 1) * LANES] = rows_ref[m].astype(BF16)


def served(pieces):
    piece = pl.BlockSpec((AT_ONCE, PIECE, LANES), lambda j, at: (j, 0, 0))
    out = pl.BlockSpec((BLOCK, AT_ONCE * LANES), lambda j, at: (0, j))
    return pl.pallas_call(
        serve_kernel,
        out_shape=[jax.ShapeDtypeStruct((BLOCK, D), BF16)] * 3,
        grid_spec=pltpu.PrefetchScalarGridSpec(
            num_scalar_prefetch=1,
            grid=(SPANS // AT_ONCE,),
            in_specs=[piece] * (2 * X),
            out_specs=[out] * 3,
            scratch_shapes=[pltpu.VMEM((3, BLOCK, LANES), F32)],
        ),
        cost_estimate=pl.CostEstimate(
            flops=10**8, bytes_accessed=2 * (2 * X * pieces[0].size + 3 * BLOCK * D), transcendentals=0
        ),
        name="serve",
    )(place("x", "core", "b"), *pieces)


def place(*axes):
    return jnp.stack([lax.axis_index(axis) for axis in axes]).astype(jnp.int32)


def traded(first, second):
    low = lax.axis_index("b") == 0
    keep, send = jnp.where(low, first, second), jnp.where(low, second, first)
    got = from_peer(send, "b", B, 1)
    return jnp.where(low, keep, got), jnp.where(low, got, keep)


def far_zq(tokens):
    return jnp.stack([tokens, from_peer(tokens, "zq", ZQ, 2)])


def near_zq(two):
    return jnp.concatenate([two, from_peer(two, "zq", ZQ, 1)])


def summed(by_y):
    send = jnp.sum(by_y[:, ZQ // 2 :].astype(F32), axis=0).astype(BF16)
    got = from_peer(send, "zq", ZQ, 1)
    kept = jnp.sum(by_y[:, : ZQ // 2].astype(F32), axis=0) + got.astype(F32)
    return kept[0] + from_peer(kept[1].astype(BF16), "zq", ZQ, 2).astype(F32)


def stepped(tokens, total):
    return (tokens.astype(F32) + 0.5 * FF ** (-0.5) * total).astype(BF16)


def local(prompt, gain_pre, gate_pre, up_pre, down_pre, gain_post, gate_post, up_post, down_post):
    half = prompt.shape[0] // B
    turned = prompt.T
    parts = by_block(
        [
            ((gain_pre[:, None] * gate_pre).astype(BF16), (gain_pre[:, None] * up_pre).astype(BF16), down_pre.astype(BF16)),
            ((gain_post[:, None] * gate_post).astype(BF16), (gain_post[:, None] * up_post).astype(BF16), down_post.astype(BF16)),
        ]
    )
    tokens = jnp.stack(traded(turned[:, :half], turned[:, half:]))
    parts, wide = lax.optimization_barrier((parts, far_zq(tokens)))
    one, two = by_span(parts)
    one = paired(one)
    pieces = over_x(one)
    wide = near_zq(after(wide, one))
    wide = share(wide, "y", Y)
    two = paired(after(two, one))
    pieces += over_core(pieces)
    wide, two, *pieces = lax.optimization_barrier((wide, two, *pieces))
    partial = half_partial(wide, pieces)
    partial, two, *pieces = lax.optimization_barrier((partial, two, *pieces))
    first = served(pieces)
    pieces = over_x(two)
    by_y = swap(partial, "y")
    total, *first = lax.optimization_barrier((summed(by_y), *first))
    total, *pieces = lax.optimization_barrier((total, *pieces))
    middle = stepped(tokens, total)
    pieces += over_core(pieces)

    partial = half_partial(share(near_zq(far_zq(middle)), "y", Y), pieces)
    partial, *pieces = lax.optimization_barrier((partial, *pieces))
    second = served(pieces)
    by_y, *second = lax.optimization_barrier((swap(partial, "y"), *second))
    result = stepped(middle, summed(by_y))
    back = jnp.concatenate(traded(result[0], result[1]), axis=1)
    return (back.T, *first, *second)


def solution(mesh):
    fine = Mesh(mesh.devices.reshape(GR, ZQ, B, Y, X, CORE), AXES)
    tokens = P(("gr", "x", "core"), ("zq", "b", "y"))
    gain = P(("gr", "zq", "b", "y"))
    trained = P(("gr", "zq", "b", "y"), ("x", "core"))
    rows = P(("zq", "b", "y"), None)
    return jax.shard_map(
        local,
        mesh=fine,
        in_specs=(tokens, gain, trained, trained, trained, gain, trained, trained, trained),
        out_specs=(tokens,) + (rows,) * 6,
        check_vma=False,
    )
```

```python
import jax
import jax.numpy as jnp
from jax import lax
from jax.experimental import pallas as pl
from jax.experimental.pallas import tpu as pltpu
from jax.sharding import Mesh
from jax.sharding import PartitionSpec as P

D = 2048
FF = 5632
NORM_EPS = 1e-06
GR, ZQ, B, Y, X, CORE = 2, 4, 2, 4, 4, 2
AXES = ("gr", "zq", "b", "y", "x", "core")
ZL = ZQ * B
F32, BF16 = jnp.float32, jnp.bfloat16
BLOCK = FF // (ZL * Y)
ROWS = D // (GR * ZL * Y)
PART = BLOCK // X
PADDED = 48
LANES = Y * ROWS
SPANS = GR * ZL
PIECE = 3 * PADDED
FEATS = D // (ZL * Y)
AT_ONCE = 4


def swap(blocks, axis):
    return lax.all_to_all(blocks, axis, split_axis=0, concat_axis=0, tiled=True)


def share(block, axis, size):
    return swap(jnp.broadcast_to(block[None], (size, *block.shape)), axis)


def from_peer(block, axis, size, flip):
    return lax.ppermute(block, axis, [(i, i ^ flip) for i in range(size)])


def after(value, *others):
    return lax.optimization_barrier((value, *others))[0]


def pack_kernel(gain_ref, gate_ref, up_ref, down_ref, gain2_ref, gate2_ref, up2_ref, down2_ref, out_ref, row_ref):
    sources = (
        (gain_ref, gate_ref), (gain_ref, up_ref), (None, down_ref),
        (gain2_ref, gate2_ref), (gain2_ref, up2_ref), (None, down2_ref),
    )
    for peer in range(Y * X):
        for n, (gain, ref) in enumerate(sources):
            cols = ref[:, peer * PART : (peer + 1) * PART]
            row_ref[:, n * PART : (n + 1) * PART] = cols if gain is None else gain[...] * cols
        out_ref[peer] = row_ref[...].astype(BF16)


def packed(layers):
    arrays = [a for gain, *matrices in layers for a in (gain[:, None], *matrices)]
    vmem = pl.BlockSpec(memory_space=pltpu.VMEM)
    width = 3 * len(layers) * PART
    return pl.pallas_call(
        pack_kernel,
        out_shape=jax.ShapeDtypeStruct((Y * X, ROWS, width), BF16),
        in_specs=[vmem] * len(arrays),
        out_specs=vmem,
        scratch_shapes=[pltpu.VMEM((ROWS, width), F32)],
        cost_estimate=pl.CostEstimate(flops=10**6, bytes_accessed=10**6, transcendentals=0),
        name="pack",
    )(*arrays)


def by_block(to_yx):
    here = swap(to_yx, ("y", "x")).reshape(Y, X, ROWS, -1)
    turned = here.transpose(1, 3, 0, 2).reshape(X, -1, PART, LANES)
    return jnp.pad(turned, ((0, 0), (0, 0), (0, PADDED - PART), (0, 0))).reshape(X, -1, LANES)


def by_span(parts):
    to_z = jnp.broadcast_to(parts[None], (GR, *parts.shape)).reshape(GR * ZQ, *parts.shape[1:])
    here = swap(to_z, ("gr", "zq"))
    return [here[:, i : i + PIECE] for i in range(0, here.shape[1], PIECE)]


def paired(piece):
    near = from_peer(piece, "b", B, 1)
    low = lax.axis_index("b") == 0
    both = jnp.stack([jnp.where(low, piece, near), jnp.where(low, near, piece)], axis=1)
    return both.reshape(SPANS, PIECE, LANES)


def over_x(pair):
    return [pair] + [from_peer(pair, "x", X, k) for k in range(1, X)]


def over_core(pieces):
    return [from_peer(piece, "core", CORE, 1) for piece in pieces]


def slot(zl, zq):
    k = (zl // B) ^ zq
    return ((k & 1) << 1) | (k >> 1), zl % B


def half_kernel(at_ref, x_ref, *refs):
    piece_refs, (out_ref, acc_ref, sq_ref) = refs[: 2 * X], refs[2 * X :]
    width = x_ref.shape[-1]
    pieces = 2 * X
    zq = at_ref[0]

    def rows(span, lo, hi):
        return jnp.concatenate([ref[span, lo:hi, :] for ref in piece_refs], axis=0)

    def both(zl, lo, hi):
        return jnp.concatenate([rows(2 * zl, lo, hi), rows(2 * zl + 1, lo, hi)], axis=1)

    acc_ref[...] = jnp.zeros_like(acc_ref)
    sq_ref[...] = jnp.zeros_like(sq_ref)

    def inward(z, _):
        k, _ = slot(z * B, zq)
        tokens = jnp.concatenate([x_ref[:, k, b].reshape(Y * FEATS, width) for b in range(B)], axis=0)
        wide = tokens.astype(F32)
        sq_ref[...] += jnp.sum((wide * wide).reshape(B * Y * FEATS // 8, 8, width), axis=0)
        weights = jnp.concatenate([both(z * B + b, 0, 2 * PADDED) for b in range(B)], axis=1)
        acc_ref[...] += jnp.dot(weights, tokens, preferred_element_type=F32)
        return 0

    lax.fori_loop(0, ZQ, inward, 0)
    squares = jnp.sum(sq_ref[...], axis=0, keepdims=True)
    scale = lax.rsqrt(squares / D + NORM_EPS) * D ** (-0.5)
    sums = acc_ref[...].reshape(pieces, 2 * PADDED, width)
    gate = sums[:, :PADDED].reshape(pieces * PADDED, width) * scale
    up = sums[:, PADDED:].reshape(pieces * PADDED, width) * scale
    hidden = (gate / (1.0 + jnp.exp(-gate)) * up).astype(BF16)

    def outward(zl, _):
        part = lax.dot_general(
            both(zl, 2 * PADDED, PIECE), hidden, (((0,), (0,)), ((), ())), preferred_element_type=F32
        )
        k, b = slot(zl, zq)
        out_ref[:, k, b] = part.astype(BF16).reshape(Y, FEATS, width)
        return 0

    lax.fori_loop(0, ZL, outward, 0)


def half_partial(tokens, pieces):
    width = tokens.shape[-1]
    vmem = pl.BlockSpec(memory_space=pltpu.VMEM)
    flops = 2 * 3 * 2 * X * PADDED * D * width
    return pl.pallas_call(
        half_kernel,
        out_shape=jax.ShapeDtypeStruct(tokens.shape, BF16),
        in_specs=[pl.BlockSpec(memory_space=pltpu.SMEM)] + [vmem] * (1 + 2 * X),
        out_specs=vmem,
        scratch_shapes=[pltpu.VMEM((2 * X * 2 * PADDED, width), F32), pltpu.VMEM((8, width), F32)],
        cost_estimate=pl.CostEstimate(
            flops=flops, bytes_accessed=2 * (2 * tokens.size + 2 * X * pieces[0].size), transcendentals=0
        ),
        name="half_step",
    )(place("zq"), tokens, *pieces)


def serve_kernel(at_ref, *refs):
    piece_refs, out_refs, rows_ref = refs[: 2 * X], refs[2 * X : -1], refs[-1]
    x, here = at_ref[0], at_ref[1] == at_ref[2]
    odd, high = (x & 1) == 1, (x & 2) == 2
    for span in range(AT_ONCE):
        for m, out_ref in enumerate(out_refs):
            lo, hi = m * PADDED, (m + 1) * PADDED
            mine = [ref[span, lo:hi, :].astype(F32) for ref in piece_refs[:X]]
            other = [ref[span, lo:hi, :].astype(F32) for ref in piece_refs[X:]]
            p = [jnp.where(here, a, b) for a, b in zip(mine, other)]
            p = [jnp.where(odd, p[k ^ 1], p[k]) for k in range(X)]
            p = [jnp.where(high, p[k ^ 2], p[k]) for k in range(X)]
            for k in range(X):
                rows_ref[m, k * PART : (k + 1) * PART, :] = p[k][:PART]
            out_ref[:, span * LANES : (span + 1) * LANES] = rows_ref[m].astype(BF16)


def served(pieces):
    piece = pl.BlockSpec((AT_ONCE, PIECE, LANES), lambda j, at: (j, 0, 0))
    out = pl.BlockSpec((BLOCK, AT_ONCE * LANES), lambda j, at: (0, j))
    return pl.pallas_call(
        serve_kernel,
        out_shape=[jax.ShapeDtypeStruct((BLOCK, D), BF16)] * 3,
        grid_spec=pltpu.PrefetchScalarGridSpec(
            num_scalar_prefetch=1,
            grid=(SPANS // AT_ONCE,),
            in_specs=[piece] * (2 * X),
            out_specs=[out] * 3,
            scratch_shapes=[pltpu.VMEM((3, BLOCK, LANES), F32)],
        ),
        cost_estimate=pl.CostEstimate(
            flops=10**8, bytes_accessed=2 * (2 * X * pieces[0].size + 3 * BLOCK * D), transcendentals=0
        ),
        name="serve",
    )(place("x", "core", "b"), *pieces)


def place(*axes):
    return jnp.stack([lax.axis_index(axis) for axis in axes]).astype(jnp.int32)


def traded(first, second):
    low = lax.axis_index("b") == 0
    keep, send = jnp.where(low, first, second), jnp.where(low, second, first)
    got = from_peer(send, "b", B, 1)
    return jnp.where(low, keep, got), jnp.where(low, got, keep)


def far_zq(tokens):
    return jnp.stack([tokens, from_peer(tokens, "zq", ZQ, 2)])


def near_zq(two):
    return jnp.concatenate([two, from_peer(two, "zq", ZQ, 1)])


def summed(by_y):
    send = jnp.sum(by_y[:, ZQ // 2 :].astype(F32), axis=0).astype(BF16)
    got = from_peer(send, "zq", ZQ, 1)
    kept = jnp.sum(by_y[:, : ZQ // 2].astype(F32), axis=0) + got.astype(F32)
    return kept[0] + from_peer(kept[1].astype(BF16), "zq", ZQ, 2).astype(F32)


def stepped(tokens, total):
    return (tokens.astype(F32) + 0.5 * FF ** (-0.5) * total).astype(BF16)


def local(prompt, gain_pre, gate_pre, up_pre, down_pre, gain_post, gate_post, up_post, down_post):
    half = prompt.shape[0] // B
    turned = prompt.T
    parts = by_block(
        packed([(gain_pre, gate_pre, up_pre, down_pre), (gain_post, gate_post, up_post, down_post)])
    )
    tokens = jnp.stack(traded(turned[:, :half], turned[:, half:]))
    parts, wide = lax.optimization_barrier((parts, far_zq(tokens)))
    one, two = by_span(parts)
    wide = after(wide, one)
    one = paired(one)
    wide = near_zq(wide)
    pieces = over_x(one)
    wide = share(wide, "y", Y)
    two = paired(after(two, one))
    pieces += over_core(pieces)
    wide, two, *pieces = lax.optimization_barrier((wide, two, *pieces))
    partial = half_partial(wide, pieces)
    partial, two, *pieces = lax.optimization_barrier((partial, two, *pieces))
    first = served(pieces)
    pieces = over_x(two)
    by_y = swap(partial, "y")
    total, *first = lax.optimization_barrier((summed(by_y), *first))
    total, *pieces = lax.optimization_barrier((total, *pieces))
    middle = stepped(tokens, total)
    pieces += over_core(pieces)

    partial = half_partial(share(near_zq(far_zq(middle)), "y", Y), pieces)
    partial, *pieces = lax.optimization_barrier((partial, *pieces))
    second = served(pieces)
    by_y, *second = lax.optimization_barrier((swap(partial, "y"), *second))
    result = stepped(middle, summed(by_y))
    back = jnp.concatenate(traded(result[0], result[1]), axis=1)
    return (back.T, *first, *second)


def solution(mesh):
    fine = Mesh(mesh.devices.reshape(GR, ZQ, B, Y, X, CORE), AXES)
    tokens = P(("gr", "x", "core"), ("zq", "b", "y"))
    gain = P(("gr", "zq", "b", "y"))
    trained = P(("gr", "zq", "b", "y"), ("x", "core"))
    rows = P(("zq", "b", "y"), None)
    return jax.shard_map(
        local,
        mesh=fine,
        in_specs=(tokens, gain, trained, trained, trained, gain, trained, trained, trained),
        out_specs=(tokens,) + (rows,) * 6,
        check_vma=False,
    )
```

```python
import jax
import jax.numpy as jnp
from jax import lax
from jax.experimental import pallas as pl
from jax.experimental.pallas import tpu as pltpu
from jax.sharding import Mesh
from jax.sharding import PartitionSpec as P

D = 2048
FF = 5632
NORM_EPS = 1e-06
GR, ZQ, B, Y, X, CORE = 2, 4, 2, 4, 4, 2
AXES = ("gr", "zq", "b", "y", "x", "core")
ZL = ZQ * B
F32, BF16 = jnp.float32, jnp.bfloat16
BLOCK = FF // (ZL * Y)
ROWS = D // (GR * ZL * Y)
PART = BLOCK // X
PADDED = 48
LANES = Y * ROWS
SPANS = GR * ZL
PIECE = 3 * PADDED
FEATS = D // (ZL * Y)
AT_ONCE = 4
BUFFERS = 4
MIB = 2**20


def swap(blocks, axis):
    return lax.all_to_all(blocks, axis, split_axis=0, concat_axis=0, tiled=True)


def share(block, axis, size):
    return swap(jnp.broadcast_to(block[None], (size, *block.shape)), axis)


def from_peer(block, axis, size, flip):
    return lax.ppermute(block, axis, [(i, i ^ flip) for i in range(size)])


def after(value, *others):
    return lax.optimization_barrier((value, *others))[0]


def pack_kernel(gain_ref, gate_ref, up_ref, down_ref, gain2_ref, gate2_ref, up2_ref, down2_ref, out_ref, row_ref):
    sources = (
        (gain_ref, gate_ref), (gain_ref, up_ref), (None, down_ref),
        (gain2_ref, gate2_ref), (gain2_ref, up2_ref), (None, down2_ref),
    )
    shape = (ROWS, ROWS)
    diagonal = lax.broadcasted_iota(jnp.int32, shape, 0) == lax.broadcasted_iota(jnp.int32, shape, 1)

    def column(gain):
        return jnp.sum(jnp.where(diagonal, jnp.broadcast_to(gain[...], shape), 0.0), axis=1, keepdims=True)

    gains = {id(gain): column(gain) for gain in (gain_ref, gain2_ref)}
    for peer in range(Y * X):
        row = row_ref.at[peer % BUFFERS]
        for n, (gain, ref) in enumerate(sources):
            cols = ref[:, peer * PART : (peer + 1) * PART]
            row[:, n * PART : (n + 1) * PART] = cols if gain is None else gains[id(gain)] * cols
        out_ref[peer] = row[...].astype(BF16)


def packed(layers):
    arrays = [a for gain, *matrices in layers for a in (gain[None, :], *matrices)]
    vmem = pl.BlockSpec(memory_space=pltpu.VMEM)
    width = 3 * len(layers) * PART
    return pl.pallas_call(
        pack_kernel,
        out_shape=jax.ShapeDtypeStruct((Y * X, ROWS, width), BF16),
        in_specs=[vmem] * len(arrays),
        out_specs=vmem,
        scratch_shapes=[pltpu.VMEM((BUFFERS, ROWS, width), F32)],
        cost_estimate=pl.CostEstimate(flops=10**6, bytes_accessed=10**6, transcendentals=0),
        compiler_params=pltpu.CompilerParams(vmem_limit_bytes=8 * MIB),
        name="pack",
    )(*arrays)


def by_block(to_yx):
    here = swap(to_yx, ("y", "x")).reshape(Y, X, ROWS, -1)
    turned = here.transpose(1, 3, 0, 2).reshape(X, -1, PART, LANES)
    return jnp.pad(turned, ((0, 0), (0, 0), (0, PADDED - PART), (0, 0))).reshape(X, -1, LANES)


def by_span(parts):
    to_z = jnp.broadcast_to(parts[None], (GR, *parts.shape)).reshape(GR * ZQ, *parts.shape[1:])
    here = swap(to_z, ("gr", "zq"))
    return [here[:, i : i + PIECE] for i in range(0, here.shape[1], PIECE)]


def paired(piece):
    near = from_peer(piece, "b", B, 1)
    low = lax.axis_index("b") == 0
    both = jnp.stack([jnp.where(low, piece, near), jnp.where(low, near, piece)], axis=1)
    return both.reshape(SPANS, PIECE, LANES)


def over_x(pair):
    one, three = (from_peer(pair, "x", X, k) for k in (1, 3))
    two = from_peer(pair, "x", X, 2)
    return [pair, one, two, three]


def over_core(pieces):
    own, one, three = (from_peer(pieces[k], "core", CORE, 1) for k in (0, 1, 3))
    two = from_peer(pieces[2], "core", CORE, 1)
    return [own, one, two, three]


def slot(zl, zq):
    k = (zl // B) ^ zq
    return ((k & 1) << 1) | (k >> 1), zl % B


def half_kernel(at_ref, x_ref, *refs):
    piece_refs, (out_ref, acc_ref, sq_ref) = refs[: 2 * X], refs[2 * X :]
    width = x_ref.shape[-1]
    pieces = 2 * X
    zq = at_ref[0]

    def rows(span, lo, hi):
        return jnp.concatenate([ref[span, lo:hi, :] for ref in piece_refs], axis=0)

    def both(zl, lo, hi):
        return jnp.concatenate([rows(2 * zl, lo, hi), rows(2 * zl + 1, lo, hi)], axis=1)

    acc_ref[...] = jnp.zeros_like(acc_ref)
    sq_ref[...] = jnp.zeros_like(sq_ref)

    def inward(z, _):
        k, _ = slot(z * B, zq)
        tokens = jnp.concatenate([x_ref[:, k, b].reshape(Y * FEATS, width) for b in range(B)], axis=0)
        wide = tokens.astype(F32)
        sq_ref[...] += jnp.sum((wide * wide).reshape(B * Y * FEATS // 8, 8, width), axis=0)
        weights = jnp.concatenate([both(z * B + b, 0, 2 * PADDED) for b in range(B)], axis=1)
        acc_ref[...] += jnp.dot(weights, tokens, preferred_element_type=F32)
        return 0

    lax.fori_loop(0, ZQ, inward, 0)
    squares = jnp.sum(sq_ref[...], axis=0, keepdims=True)
    scale = lax.rsqrt(squares / D + NORM_EPS) * D ** (-0.5)
    sums = acc_ref[...].reshape(pieces, 2 * PADDED, width)
    gate = sums[:, :PADDED].reshape(pieces * PADDED, width) * scale
    up = sums[:, PADDED:].reshape(pieces * PADDED, width) * scale
    hidden = (gate / (1.0 + jnp.exp(-gate)) * up).astype(BF16)

    def outward(zl, _):
        part = lax.dot_general(
            both(zl, 2 * PADDED, PIECE), hidden, (((0,), (0,)), ((), ())), preferred_element_type=F32
        )
        k, b = slot(zl, zq)
        out_ref[:, k, b] = part.astype(BF16).reshape(Y, FEATS, width)
        return 0

    lax.fori_loop(0, ZL, outward, 0)


def half_partial(tokens, pieces):
    width = tokens.shape[-1]
    vmem = pl.BlockSpec(memory_space=pltpu.VMEM)
    flops = 2 * 3 * 2 * X * PADDED * D * width
    return pl.pallas_call(
        half_kernel,
        out_shape=jax.ShapeDtypeStruct(tokens.shape, BF16),
        in_specs=[pl.BlockSpec(memory_space=pltpu.SMEM)] + [vmem] * (1 + 2 * X),
        out_specs=vmem,
        scratch_shapes=[pltpu.VMEM((2 * X * 2 * PADDED, width), F32), pltpu.VMEM((8, width), F32)],
        cost_estimate=pl.CostEstimate(
            flops=flops, bytes_accessed=2 * (2 * tokens.size + 2 * X * pieces[0].size), transcendentals=0
        ),
        compiler_params=pltpu.CompilerParams(vmem_limit_bytes=20 * MIB),
        name="half_step",
    )(place("zq"), tokens, *pieces)


def serve_kernel(at_ref, *refs):
    piece_refs, out_refs, rows_ref = refs[: 2 * X], refs[2 * X : -1], refs[-1]
    x, here = at_ref[0], at_ref[1] == at_ref[2]
    odd, high = (x & 1) == 1, (x & 2) == 2
    for span in range(AT_ONCE):
        for m, out_ref in enumerate(out_refs):
            lo, hi = m * PADDED, (m + 1) * PADDED
            mine = [ref[span, lo:hi, :].astype(F32) for ref in piece_refs[:X]]
            other = [ref[span, lo:hi, :].astype(F32) for ref in piece_refs[X:]]
            p = [jnp.where(here, a, b) for a, b in zip(mine, other)]
            p = [jnp.where(odd, p[k ^ 1], p[k]) for k in range(X)]
            p = [jnp.where(high, p[k ^ 2], p[k]) for k in range(X)]
            for k in range(X):
                rows_ref[m, k * PART : (k + 1) * PART, :] = p[k][:PART]
            out_ref[:, span * LANES : (span + 1) * LANES] = rows_ref[m].astype(BF16)


def served(pieces):
    piece = pl.BlockSpec((AT_ONCE, PIECE, LANES), lambda j, at: (j, 0, 0))
    out = pl.BlockSpec((BLOCK, AT_ONCE * LANES), lambda j, at: (0, j))
    return pl.pallas_call(
        serve_kernel,
        out_shape=[jax.ShapeDtypeStruct((BLOCK, D), BF16)] * 3,
        grid_spec=pltpu.PrefetchScalarGridSpec(
            num_scalar_prefetch=1,
            grid=(SPANS // AT_ONCE,),
            in_specs=[piece] * (2 * X),
            out_specs=[out] * 3,
            scratch_shapes=[pltpu.VMEM((3, BLOCK, LANES), F32)],
        ),
        cost_estimate=pl.CostEstimate(
            flops=10**8, bytes_accessed=2 * (2 * X * pieces[0].size + 3 * BLOCK * D), transcendentals=0
        ),
        compiler_params=pltpu.CompilerParams(vmem_limit_bytes=16 * MIB),
        name="serve",
    )(place("x", "core", "b"), *pieces)


def place(*axes):
    return jnp.stack([lax.axis_index(axis) for axis in axes]).astype(jnp.int32)


def traded(first, second):
    low = lax.axis_index("b") == 0
    keep, send = jnp.where(low, first, second), jnp.where(low, second, first)
    got = from_peer(send, "b", B, 1)
    return jnp.where(low, keep, got), jnp.where(low, got, keep)


def far_zq(tokens):
    return jnp.stack([tokens, from_peer(tokens, "zq", ZQ, 2)])


def near_zq(two):
    return jnp.concatenate([two, from_peer(two, "zq", ZQ, 1)])


def summed(by_y):
    send = jnp.sum(by_y[:, ZQ // 2 :].astype(F32), axis=0).astype(BF16)
    got = from_peer(send, "zq", ZQ, 1)
    kept = jnp.sum(by_y[:, : ZQ // 2].astype(F32), axis=0) + got.astype(F32)
    return kept[0] + from_peer(kept[1].astype(BF16), "zq", ZQ, 2).astype(F32)


def stepped(tokens, total):
    return (tokens.astype(F32) + 0.5 * FF ** (-0.5) * total).astype(BF16)


def local(prompt, gain_pre, gate_pre, up_pre, down_pre, gain_post, gate_post, up_post, down_post):
    half = prompt.shape[0] // B
    turned = prompt.T
    parts = by_block(
        packed([(gain_pre, gate_pre, up_pre, down_pre), (gain_post, gate_post, up_post, down_post)])
    )
    tokens = jnp.stack(traded(turned[:, :half], turned[:, half:]))
    parts, wide = lax.optimization_barrier((parts, far_zq(tokens)))
    one, two = by_span(parts)
    wide = after(wide, one)
    one = paired(one)
    wide = near_zq(wide)
    pieces = over_x(one)
    wide = share(wide, "y", Y)
    two = paired(after(two, one))
    pieces += over_core(pieces)
    wide, two, *pieces = lax.optimization_barrier((wide, two, *pieces))
    partial = half_partial(wide, pieces)
    partial, two, *pieces = lax.optimization_barrier((partial, two, *pieces))
    first = served(pieces)
    pieces = over_x(two)
    by_y = swap(partial, "y")
    total, *first = lax.optimization_barrier((summed(by_y), *first))
    total, *pieces = lax.optimization_barrier((total, *pieces))
    middle = stepped(tokens, total)
    pieces += over_core(pieces)

    partial = half_partial(share(near_zq(far_zq(middle)), "y", Y), pieces)
    partial, *pieces = lax.optimization_barrier((partial, *pieces))
    second = served(pieces)
    by_y, *second = lax.optimization_barrier((swap(partial, "y"), *second))
    result = stepped(middle, summed(by_y))
    back = jnp.concatenate(traded(result[0], result[1]), axis=1)
    return (back.T, *first, *second)


def solution(mesh):
    fine = Mesh(mesh.devices.reshape(GR, ZQ, B, Y, X, CORE), AXES)
    tokens = P(("gr", "x", "core"), ("zq", "b", "y"))
    gain = P(("gr", "zq", "b", "y"))
    trained = P(("gr", "zq", "b", "y"), ("x", "core"))
    rows = P(("zq", "b", "y"), None)
    return jax.shard_map(
        local,
        mesh=fine,
        in_specs=(tokens, gain, trained, trained, trained, gain, trained, trained, trained),
        out_specs=(tokens,) + (rows,) * 6,
        check_vma=False,
    )
```

```python
import jax
import jax.numpy as jnp
from jax import lax
from jax.experimental import pallas as pl
from jax.experimental.pallas import tpu as pltpu
from jax.sharding import Mesh
from jax.sharding import PartitionSpec as P

D = 2048
FF = 5632
NORM_EPS = 1e-06
GR, ZQ, B, Y, X, CORE = 2, 4, 2, 4, 4, 2
AXES = ("gr", "zq", "b", "y", "x", "core")
ZL = ZQ * B
F32, BF16 = jnp.float32, jnp.bfloat16
BLOCK = FF // (ZL * Y)
ROWS = D // (GR * ZL * Y)
PART = BLOCK // X
PADDED = 48
LANES = Y * ROWS
SPANS = GR * ZL
PIECE = 3 * PADDED
FEATS = D // (ZL * Y)
AT_ONCE = 4
BUFFERS = 4
MIB = 2**20


def swap(blocks, axis):
    return lax.all_to_all(blocks, axis, split_axis=0, concat_axis=0, tiled=True)


def share(block, axis, size):
    return swap(jnp.broadcast_to(block[None], (size, *block.shape)), axis)


def from_peer(block, axis, size, flip):
    return lax.ppermute(block, axis, [(i, i ^ flip) for i in range(size)])


def after(value, *others):
    return lax.optimization_barrier((value, *others))[0]


def pack_kernel(gain_ref, gain2_ref, *refs):
    inputs, (out_ref, held_ref, row_ref, sems) = refs[:-4], refs[-4:]
    copies = [pltpu.make_async_copy(ref, held_ref.at[n], sems.at[n]) for n, ref in enumerate(inputs)]
    for copy in copies:
        copy.start()
    shape = (ROWS, ROWS)
    diagonal = lax.broadcasted_iota(jnp.int32, shape, 0) == lax.broadcasted_iota(jnp.int32, shape, 1)

    def column(gain):
        return jnp.sum(jnp.where(diagonal, jnp.broadcast_to(gain[...], shape), 0.0), axis=1, keepdims=True)

    first, second = column(gain_ref), column(gain2_ref)
    gains = (first, first, None, second, second, None)
    for copy in copies:
        copy.wait()
    for peer in range(Y * X):
        row = row_ref.at[peer % BUFFERS]
        for n, gain in enumerate(gains):
            cols = held_ref[n, :, peer * PART : (peer + 1) * PART]
            row[:, n * PART : (n + 1) * PART] = cols if gain is None else gain * cols
        out_ref[peer] = row[...].astype(BF16)


def packed(layers):
    gains = [layer[0][None, :] for layer in layers]
    matrices = [matrix for layer in layers for matrix in layer[1:]]
    vmem = pl.BlockSpec(memory_space=pltpu.VMEM)
    width = len(matrices) * PART
    return pl.pallas_call(
        pack_kernel,
        out_shape=jax.ShapeDtypeStruct((Y * X, ROWS, width), BF16),
        in_specs=[vmem] * len(gains) + [pl.BlockSpec(memory_space=pl.ANY)] * len(matrices),
        out_specs=vmem,
        scratch_shapes=[
            pltpu.VMEM((len(matrices), *matrices[0].shape), F32),
            pltpu.VMEM((BUFFERS, ROWS, width), F32),
            pltpu.SemaphoreType.DMA((len(matrices),)),
        ],
        cost_estimate=pl.CostEstimate(flops=10**6, bytes_accessed=10**6, transcendentals=0),
        name="pack",
    )(*gains, *matrices)


def by_block(to_yx):
    here = swap(to_yx, ("y", "x")).reshape(Y, X, ROWS, -1)
    turned = here.transpose(1, 3, 0, 2).reshape(X, -1, PART, LANES)
    return jnp.pad(turned, ((0, 0), (0, 0), (0, PADDED - PART), (0, 0))).reshape(X, -1, LANES)


def by_span(parts):
    to_z = jnp.broadcast_to(parts[None], (GR, *parts.shape)).reshape(GR * ZQ, *parts.shape[1:])
    here = swap(to_z, ("gr", "zq"))
    return [here[:, i : i + PIECE] for i in range(0, here.shape[1], PIECE)]


def paired(piece):
    near = from_peer(piece, "b", B, 1)
    low = lax.axis_index("b") == 0
    both = jnp.stack([jnp.where(low, piece, near), jnp.where(low, near, piece)], axis=1)
    return both.reshape(SPANS, PIECE, LANES)


def over_x(pair):
    one, three = (from_peer(pair, "x", X, k) for k in (1, 3))
    two = from_peer(pair, "x", X, 2)
    return [pair, one, two, three]


def over_core(pieces):
    own, one, three = (from_peer(pieces[k], "core", CORE, 1) for k in (0, 1, 3))
    two = from_peer(pieces[2], "core", CORE, 1)
    return [own, one, two, three]


def slot(zl, zq):
    k = (zl // B) ^ zq
    return ((k & 1) << 1) | (k >> 1), zl % B


def half_kernel(at_ref, x_ref, *refs):
    piece_refs, (out_ref, acc_ref, sq_ref) = refs[: 2 * X], refs[2 * X :]
    width = x_ref.shape[-1]
    pieces = 2 * X
    zq = at_ref[0]

    def rows(span, lo, hi):
        return jnp.concatenate([ref[span, lo:hi, :] for ref in piece_refs], axis=0)

    def both(zl, lo, hi):
        return jnp.concatenate([rows(2 * zl, lo, hi), rows(2 * zl + 1, lo, hi)], axis=1)

    acc_ref[...] = jnp.zeros_like(acc_ref)
    sq_ref[...] = jnp.zeros_like(sq_ref)

    def inward(z, _):
        k, _ = slot(z * B, zq)
        tokens = jnp.concatenate([x_ref[:, k, b].reshape(Y * FEATS, width) for b in range(B)], axis=0)
        wide = tokens.astype(F32)
        sq_ref[...] += jnp.sum((wide * wide).reshape(B * Y * FEATS // 8, 8, width), axis=0)
        weights = jnp.concatenate([both(z * B + b, 0, 2 * PADDED) for b in range(B)], axis=1)
        acc_ref[...] += jnp.dot(weights, tokens, preferred_element_type=F32)
        return 0

    lax.fori_loop(0, ZQ, inward, 0)
    squares = jnp.sum(sq_ref[...], axis=0, keepdims=True)
    scale = lax.rsqrt(squares / D + NORM_EPS) * D ** (-0.5)
    sums = acc_ref[...].reshape(pieces, 2 * PADDED, width)
    gate = sums[:, :PADDED].reshape(pieces * PADDED, width) * scale
    up = sums[:, PADDED:].reshape(pieces * PADDED, width) * scale
    hidden = (gate / (1.0 + jnp.exp(-gate)) * up).astype(BF16)

    def outward(zl, _):
        part = lax.dot_general(
            both(zl, 2 * PADDED, PIECE), hidden, (((0,), (0,)), ((), ())), preferred_element_type=F32
        )
        k, b = slot(zl, zq)
        out_ref[:, k, b] = part.astype(BF16).reshape(Y, FEATS, width)
        return 0

    lax.fori_loop(0, ZL, outward, 0)


def half_partial(tokens, pieces):
    width = tokens.shape[-1]
    vmem = pl.BlockSpec(memory_space=pltpu.VMEM)
    flops = 2 * 3 * 2 * X * PADDED * D * width
    return pl.pallas_call(
        half_kernel,
        out_shape=jax.ShapeDtypeStruct(tokens.shape, BF16),
        in_specs=[pl.BlockSpec(memory_space=pltpu.SMEM)] + [vmem] * (1 + 2 * X),
        out_specs=vmem,
        scratch_shapes=[pltpu.VMEM((2 * X * 2 * PADDED, width), F32), pltpu.VMEM((8, width), F32)],
        cost_estimate=pl.CostEstimate(
            flops=flops, bytes_accessed=2 * (2 * tokens.size + 2 * X * pieces[0].size), transcendentals=0
        ),
        compiler_params=pltpu.CompilerParams(vmem_limit_bytes=20 * MIB),
        name="half_step",
    )(place("zq"), tokens, *pieces)


def serve_kernel(at_ref, *refs):
    piece_refs, out_refs, rows_ref = refs[: 2 * X], refs[2 * X : -1], refs[-1]
    x, here = at_ref[0], at_ref[1] == at_ref[2]
    odd, high = (x & 1) == 1, (x & 2) == 2
    for span in range(AT_ONCE):
        for m, out_ref in enumerate(out_refs):
            lo, hi = m * PADDED, (m + 1) * PADDED
            mine = [ref[span, lo:hi, :].astype(F32) for ref in piece_refs[:X]]
            other = [ref[span, lo:hi, :].astype(F32) for ref in piece_refs[X:]]
            p = [jnp.where(here, a, b) for a, b in zip(mine, other)]
            p = [jnp.where(odd, p[k ^ 1], p[k]) for k in range(X)]
            p = [jnp.where(high, p[k ^ 2], p[k]) for k in range(X)]
            for k in range(X):
                rows_ref[m, k * PART : (k + 1) * PART, :] = p[k][:PART]
            out_ref[:, span * LANES : (span + 1) * LANES] = rows_ref[m].astype(BF16)


def served(pieces):
    piece = pl.BlockSpec((AT_ONCE, PIECE, LANES), lambda j, at: (j, 0, 0))
    out = pl.BlockSpec((BLOCK, AT_ONCE * LANES), lambda j, at: (0, j))
    return pl.pallas_call(
        serve_kernel,
        out_shape=[jax.ShapeDtypeStruct((BLOCK, D), BF16)] * 3,
        grid_spec=pltpu.PrefetchScalarGridSpec(
            num_scalar_prefetch=1,
            grid=(SPANS // AT_ONCE,),
            in_specs=[piece] * (2 * X),
            out_specs=[out] * 3,
            scratch_shapes=[pltpu.VMEM((3, BLOCK, LANES), F32)],
        ),
        cost_estimate=pl.CostEstimate(
            flops=10**8, bytes_accessed=2 * (2 * X * pieces[0].size + 3 * BLOCK * D), transcendentals=0
        ),
        compiler_params=pltpu.CompilerParams(vmem_limit_bytes=16 * MIB),
        name="serve",
    )(place("x", "core", "b"), *pieces)


def place(*axes):
    return jnp.stack([lax.axis_index(axis) for axis in axes]).astype(jnp.int32)


def traded(first, second):
    low = lax.axis_index("b") == 0
    keep, send = jnp.where(low, first, second), jnp.where(low, second, first)
    got = from_peer(send, "b", B, 1)
    return jnp.where(low, keep, got), jnp.where(low, got, keep)


def far_zq(tokens):
    return jnp.stack([tokens, from_peer(tokens, "zq", ZQ, 2)])


def near_zq(two):
    return jnp.concatenate([two, from_peer(two, "zq", ZQ, 1)])


def summed(by_y):
    send = jnp.sum(by_y[:, ZQ // 2 :].astype(F32), axis=0).astype(BF16)
    got = from_peer(send, "zq", ZQ, 1)
    kept = jnp.sum(by_y[:, : ZQ // 2].astype(F32), axis=0) + got.astype(F32)
    return kept[0] + from_peer(kept[1].astype(BF16), "zq", ZQ, 2).astype(F32)


def stepped(tokens, total):
    return (tokens.astype(F32) + 0.5 * FF ** (-0.5) * total).astype(BF16)


def local(prompt, gain_pre, gate_pre, up_pre, down_pre, gain_post, gate_post, up_post, down_post):
    half = prompt.shape[0] // B
    turned = prompt.T
    parts = by_block(
        packed([(gain_pre, gate_pre, up_pre, down_pre), (gain_post, gate_post, up_post, down_post)])
    )
    tokens = jnp.stack(traded(turned[:, :half], turned[:, half:]))
    parts, wide = lax.optimization_barrier((parts, far_zq(tokens)))
    one, two = by_span(parts)
    wide = after(wide, one)
    one = paired(one)
    wide = near_zq(wide)
    pieces = over_x(one)
    wide = share(wide, "y", Y)
    two = paired(after(two, one))
    pieces += over_core(pieces)
    wide, two, *pieces = lax.optimization_barrier((wide, two, *pieces))
    partial = half_partial(wide, pieces)
    partial, two, *pieces = lax.optimization_barrier((partial, two, *pieces))
    first = served(pieces)
    pieces = over_x(two)
    by_y = swap(partial, "y")
    total, *first = lax.optimization_barrier((summed(by_y), *first))
    total, *pieces = lax.optimization_barrier((total, *pieces))
    middle = stepped(tokens, total)
    pieces += over_core(pieces)

    partial = half_partial(share(near_zq(far_zq(middle)), "y", Y), pieces)
    partial, *pieces = lax.optimization_barrier((partial, *pieces))
    second = served(pieces)
    by_y, *second = lax.optimization_barrier((swap(partial, "y"), *second))
    result = stepped(middle, summed(by_y))
    back = jnp.concatenate(traded(result[0], result[1]), axis=1)
    return (back.T, *first, *second)


def solution(mesh):
    fine = Mesh(mesh.devices.reshape(GR, ZQ, B, Y, X, CORE), AXES)
    tokens = P(("gr", "x", "core"), ("zq", "b", "y"))
    gain = P(("gr", "zq", "b", "y"))
    trained = P(("gr", "zq", "b", "y"), ("x", "core"))
    rows = P(("zq", "b", "y"), None)
    return jax.shard_map(
        local,
        mesh=fine,
        in_specs=(tokens, gain, trained, trained, trained, gain, trained, trained, trained),
        out_specs=(tokens,) + (rows,) * 6,
        check_vma=False,
    )
```

```python
import jax
import jax.numpy as jnp
from jax import lax
from jax.experimental import pallas as pl
from jax.experimental.pallas import tpu as pltpu
from jax.sharding import Mesh
from jax.sharding import PartitionSpec as P

D = 2048
FF = 5632
NORM_EPS = 1e-06
GR, ZQ, B, Y, X, CORE = 2, 4, 2, 4, 4, 2
AXES = ("gr", "zq", "b", "y", "x", "core")
ZL = ZQ * B
F32, BF16 = jnp.float32, jnp.bfloat16
BLOCK = FF // (ZL * Y)
ROWS = D // (GR * ZL * Y)
PART = BLOCK // X
PADDED = 48
LANES = Y * ROWS
SPANS = GR * ZL
PIECE = 3 * PADDED
FEATS = D // (ZL * Y)
AT_ONCE = 4
BUFFERS = 4
MIB = 2**20


def swap(blocks, axis):
    return lax.all_to_all(blocks, axis, split_axis=0, concat_axis=0, tiled=True)


def share(block, axis, size):
    return swap(jnp.broadcast_to(block[None], (size, *block.shape)), axis)


def from_peer(block, axis, size, flip):
    return lax.ppermute(block, axis, [(i, i ^ flip) for i in range(size)])


def after(value, *others):
    return lax.optimization_barrier((value, *others))[0]


def pack_kernel(gain_ref, gain2_ref, *refs):
    inputs, (out_ref, held_ref, row_ref, sems) = refs[:-4], refs[-4:]
    copies = [pltpu.make_async_copy(ref, held_ref.at[n], sems.at[n]) for n, ref in enumerate(inputs)]
    for copy in copies:
        copy.start()
    shape = (ROWS, ROWS)
    diagonal = lax.broadcasted_iota(jnp.int32, shape, 0) == lax.broadcasted_iota(jnp.int32, shape, 1)

    def column(gain):
        return jnp.sum(jnp.where(diagonal, jnp.broadcast_to(gain[...], shape), 0.0), axis=1, keepdims=True)

    first, second = column(gain_ref), column(gain2_ref)
    gains = (first, first, None, second, second, None)
    for copy in copies:
        copy.wait()
    for peer in range(Y * X):
        row = row_ref.at[peer % BUFFERS]
        for n, gain in enumerate(gains):
            cols = held_ref[n, :, peer * PART : (peer + 1) * PART]
            row[:, n * PART : (n + 1) * PART] = cols if gain is None else gain * cols
        out_ref[peer] = row[...].astype(BF16)


def packed(layers):
    gains = [layer[0][None, :] for layer in layers]
    matrices = [matrix for layer in layers for matrix in layer[1:]]
    vmem = pl.BlockSpec(memory_space=pltpu.VMEM)
    width = len(matrices) * PART
    return pl.pallas_call(
        pack_kernel,
        out_shape=jax.ShapeDtypeStruct((Y * X, ROWS, width), BF16),
        in_specs=[vmem] * len(gains) + [pl.BlockSpec(memory_space=pl.ANY)] * len(matrices),
        out_specs=vmem,
        scratch_shapes=[
            pltpu.VMEM((len(matrices), *matrices[0].shape), F32),
            pltpu.VMEM((BUFFERS, ROWS, width), F32),
            pltpu.SemaphoreType.DMA((len(matrices),)),
        ],
        cost_estimate=pl.CostEstimate(flops=10**6, bytes_accessed=10**6, transcendentals=0),
        name="pack",
    )(*gains, *matrices)


def by_block(to_yx):
    here = swap(to_yx, ("y", "x")).reshape(Y, X, ROWS, -1)
    turned = here.transpose(1, 3, 0, 2).reshape(X, -1, PART, LANES)
    return jnp.pad(turned, ((0, 0), (0, 0), (0, PADDED - PART), (0, 0))).reshape(X, -1, LANES)


def by_span(parts):
    to_z = jnp.broadcast_to(parts[None], (GR, *parts.shape)).reshape(GR * ZQ, *parts.shape[1:])
    here = swap(to_z, ("gr", "zq"))
    return [here[:, i : i + PIECE] for i in range(0, here.shape[1], PIECE)]


def paired(piece):
    near = from_peer(piece, "b", B, 1)
    low = lax.axis_index("b") == 0
    both = jnp.stack([jnp.where(low, piece, near), jnp.where(low, near, piece)], axis=1)
    return both.reshape(SPANS, PIECE, LANES)


def over_x(pair):
    one, three = (from_peer(pair, "x", X, k) for k in (1, 3))
    two = from_peer(pair, "x", X, 2)
    return [pair, one, two, three]


def over_core(pieces):
    own, one, three = (from_peer(pieces[k], "core", CORE, 1) for k in (0, 1, 3))
    two = from_peer(pieces[2], "core", CORE, 1)
    return [own, one, two, three]


def slot(zl, zq):
    k = (zl // B) ^ zq
    return ((k & 1) << 1) | (k >> 1), zl % B


def half_kernel(at_ref, x_ref, *refs):
    piece_refs, (out_ref, acc_ref, sq_ref) = refs[: 2 * X], refs[2 * X :]
    width = x_ref.shape[-1]
    pieces = 2 * X
    zq = at_ref[0]

    def rows(span, lo, hi):
        return jnp.concatenate([ref[span, lo:hi, :] for ref in piece_refs], axis=0)

    def both(zl, lo, hi):
        return jnp.concatenate([rows(2 * zl, lo, hi), rows(2 * zl + 1, lo, hi)], axis=1)

    acc_ref[...] = jnp.zeros_like(acc_ref)
    sq_ref[...] = jnp.zeros_like(sq_ref)

    def inward(z, _):
        k, _ = slot(z * B, zq)
        tokens = jnp.concatenate([x_ref[:, k, b].reshape(Y * FEATS, width) for b in range(B)], axis=0)
        wide = tokens.astype(F32)
        sq_ref[...] += jnp.sum((wide * wide).reshape(B * Y * FEATS // 8, 8, width), axis=0)
        weights = jnp.concatenate([both(z * B + b, 0, 2 * PADDED) for b in range(B)], axis=1)
        acc_ref[...] += jnp.dot(weights, tokens, preferred_element_type=F32)
        return 0

    lax.fori_loop(0, ZQ, inward, 0)
    squares = jnp.sum(sq_ref[...], axis=0, keepdims=True)
    scale = lax.rsqrt(squares / D + NORM_EPS) * D ** (-0.5)
    sums = acc_ref[...].reshape(pieces, 2 * PADDED, width)
    gate = sums[:, :PADDED].reshape(pieces * PADDED, width) * scale
    up = sums[:, PADDED:].reshape(pieces * PADDED, width) * scale
    hidden = (gate / (1.0 + jnp.exp(-gate)) * up).astype(BF16)

    def outward(zl, _):
        part = lax.dot_general(
            both(zl, 2 * PADDED, PIECE), hidden, (((0,), (0,)), ((), ())), preferred_element_type=F32
        )
        k, b = slot(zl, zq)
        out_ref[:, k, b] = part.astype(BF16).reshape(Y, FEATS, width)
        return 0

    lax.fori_loop(0, ZL, outward, 0)


def half_partial(tokens, pieces):
    width = tokens.shape[-1]
    vmem = pl.BlockSpec(memory_space=pltpu.VMEM)
    flops = 2 * 3 * 2 * X * PADDED * D * width
    return pl.pallas_call(
        half_kernel,
        out_shape=jax.ShapeDtypeStruct(tokens.shape, BF16),
        in_specs=[pl.BlockSpec(memory_space=pltpu.SMEM)] + [vmem] * (1 + 2 * X),
        out_specs=vmem,
        scratch_shapes=[pltpu.VMEM((2 * X * 2 * PADDED, width), F32), pltpu.VMEM((8, width), F32)],
        cost_estimate=pl.CostEstimate(
            flops=flops, bytes_accessed=2 * (2 * tokens.size + 2 * X * pieces[0].size), transcendentals=0
        ),
        compiler_params=pltpu.CompilerParams(vmem_limit_bytes=20 * MIB),
        name="half_step",
    )(place("zq"), tokens, *pieces)


def serve_kernel(at_ref, *refs):
    piece_refs, out_refs, rows_ref = refs[: 2 * X], refs[2 * X : -1], refs[-1]
    x, here = at_ref[0], at_ref[1] == at_ref[2]
    odd, high = (x & 1) == 1, (x & 2) == 2
    for span in range(AT_ONCE):
        for m, out_ref in enumerate(out_refs):
            lo, hi = m * PADDED, (m + 1) * PADDED
            mine = [ref[span, lo:hi, :].astype(F32) for ref in piece_refs[:X]]
            other = [ref[span, lo:hi, :].astype(F32) for ref in piece_refs[X:]]
            p = [jnp.where(here, a, b) for a, b in zip(mine, other)]
            p = [jnp.where(odd, p[k ^ 1], p[k]) for k in range(X)]
            p = [jnp.where(high, p[k ^ 2], p[k]) for k in range(X)]
            for k in range(X):
                rows_ref[m, k * PART : (k + 1) * PART, :] = p[k][:PART]
            out_ref[:, span * LANES : (span + 1) * LANES] = rows_ref[m].astype(BF16)


def served(pieces):
    piece = pl.BlockSpec((AT_ONCE, PIECE, LANES), lambda j, at: (j, 0, 0))
    out = pl.BlockSpec((BLOCK, AT_ONCE * LANES), lambda j, at: (0, j))
    return pl.pallas_call(
        serve_kernel,
        out_shape=[jax.ShapeDtypeStruct((BLOCK, D), BF16)] * 3,
        grid_spec=pltpu.PrefetchScalarGridSpec(
            num_scalar_prefetch=1,
            grid=(SPANS // AT_ONCE,),
            in_specs=[piece] * (2 * X),
            out_specs=[out] * 3,
            scratch_shapes=[pltpu.VMEM((3, BLOCK, LANES), F32)],
        ),
        cost_estimate=pl.CostEstimate(
            flops=10**8, bytes_accessed=2 * (2 * X * pieces[0].size + 3 * BLOCK * D), transcendentals=0
        ),
        compiler_params=pltpu.CompilerParams(vmem_limit_bytes=16 * MIB),
        name="serve",
    )(place("x", "core", "b"), *pieces)


def place(*axes):
    return jnp.stack([lax.axis_index(axis) for axis in axes]).astype(jnp.int32)


def traded(first, second):
    low = lax.axis_index("b") == 0
    keep, send = jnp.where(low, first, second), jnp.where(low, second, first)
    got = from_peer(send, "b", B, 1)
    return jnp.where(low, keep, got), jnp.where(low, got, keep)


def far_zq(tokens):
    return jnp.stack([tokens, from_peer(tokens, "zq", ZQ, 2)])


def near_zq(two):
    return jnp.concatenate([two, from_peer(two, "zq", ZQ, 1)])


def kept_half(by_y):
    send = jnp.sum(by_y[:, ZQ // 2 :].astype(F32), axis=0).astype(BF16)
    got = from_peer(send, "zq", ZQ, 1)
    return jnp.sum(by_y[:, : ZQ // 2].astype(F32), axis=0) + got.astype(F32)


def summed(by_y):
    kept = kept_half(by_y)
    return kept[0] + from_peer(kept[1].astype(BF16), "zq", ZQ, 2).astype(F32)


def summed_twice(by_y):
    kept = kept_half(by_y).astype(BF16)
    got = from_peer(kept, "zq", ZQ, 2)
    return kept.astype(F32) + got[::-1].astype(F32)


def stepped(tokens, total):
    return (tokens.astype(F32) + 0.5 * FF ** (-0.5) * total).astype(BF16)


def local(prompt, gain_pre, gate_pre, up_pre, down_pre, gain_post, gate_post, up_post, down_post):
    half = prompt.shape[0] // B
    turned = prompt.T
    parts = by_block(
        packed([(gain_pre, gate_pre, up_pre, down_pre), (gain_post, gate_post, up_post, down_post)])
    )
    tokens = jnp.stack(traded(turned[:, :half], turned[:, half:]))
    parts, two_away = lax.optimization_barrier((parts, far_zq(tokens)))
    one, two = by_span(parts)
    wide = after(two_away, one)
    one = paired(one)
    wide = near_zq(wide)
    pieces = over_x(one)
    wide = share(wide, "y", Y)
    two = paired(after(two, one))
    pieces += over_core(pieces)
    wide, two, *pieces = lax.optimization_barrier((wide, two, *pieces))
    partial = half_partial(wide, pieces)
    partial, two, *pieces = lax.optimization_barrier((partial, two, *pieces))
    first = served(pieces)
    pieces = over_x(two)
    by_y = swap(partial, "y")
    total, *first = lax.optimization_barrier((summed_twice(by_y), *first))
    total, *pieces = lax.optimization_barrier((total, *pieces))
    middle = stepped(two_away, total)
    pieces += over_core(pieces)

    partial = half_partial(share(near_zq(middle), "y", Y), pieces)
    partial, *pieces = lax.optimization_barrier((partial, *pieces))
    second = served(pieces)
    by_y, *second = lax.optimization_barrier((swap(partial, "y"), *second))
    result = stepped(middle[0], summed(by_y))
    back = jnp.concatenate(traded(result[0], result[1]), axis=1)
    return (back.T, *first, *second)


def solution(mesh):
    fine = Mesh(mesh.devices.reshape(GR, ZQ, B, Y, X, CORE), AXES)
    tokens = P(("gr", "x", "core"), ("zq", "b", "y"))
    gain = P(("gr", "zq", "b", "y"))
    trained = P(("gr", "zq", "b", "y"), ("x", "core"))
    rows = P(("zq", "b", "y"), None)
    return jax.shard_map(
        local,
        mesh=fine,
        in_specs=(tokens, gain, trained, trained, trained, gain, trained, trained, trained),
        out_specs=(tokens,) + (rows,) * 6,
        check_vma=False,
    )
```

```python
import jax
import jax.numpy as jnp
from jax import lax
from jax.experimental import pallas as pl
from jax.experimental.pallas import tpu as pltpu
from jax.sharding import Mesh
from jax.sharding import PartitionSpec as P

D = 2048
FF = 5632
NORM_EPS = 1e-06
GR, ZQ, B, Y, X, CORE = 2, 4, 2, 4, 4, 2
AXES = ("gr", "zq", "b", "y", "x", "core")
ZL = ZQ * B
F32, BF16 = jnp.float32, jnp.bfloat16
BLOCK = FF // (ZL * Y)
ROWS = D // (GR * ZL * Y)
PART = BLOCK // X
PADDED = 48
LANES = Y * ROWS
SPANS = GR * ZL
PIECE = 3 * PADDED
FEATS = D // (ZL * Y)
AT_ONCE = 4
BUFFERS = 4
MIB = 2**20


def swap(blocks, axis):
    return lax.all_to_all(blocks, axis, split_axis=0, concat_axis=0, tiled=True)


def share(block, axis, size):
    return swap(jnp.broadcast_to(block[None], (size, *block.shape)), axis)


def from_peer(block, axis, size, flip):
    return lax.ppermute(block, axis, [(i, i ^ flip) for i in range(size)])


def after(value, *others):
    return lax.optimization_barrier((value, *others))[0]


def pack_kernel(gain_ref, gain2_ref, *refs):
    inputs, (out_ref, held_ref, row_ref, sems) = refs[:-4], refs[-4:]
    copies = [pltpu.make_async_copy(ref, held_ref.at[n], sems.at[n]) for n, ref in enumerate(inputs)]
    for copy in copies:
        copy.start()
    shape = (ROWS, ROWS)
    diagonal = lax.broadcasted_iota(jnp.int32, shape, 0) == lax.broadcasted_iota(jnp.int32, shape, 1)

    def column(gain):
        return jnp.sum(jnp.where(diagonal, jnp.broadcast_to(gain[...], shape), 0.0), axis=1, keepdims=True)

    first, second = column(gain_ref), column(gain2_ref)
    gains = (first, first, None, second, second, None)
    for copy in copies:
        copy.wait()
    for peer in range(Y * X):
        row = row_ref.at[peer % BUFFERS]
        for n, gain in enumerate(gains):
            cols = held_ref[n, :, peer * PART : (peer + 1) * PART]
            row[:, n * PART : (n + 1) * PART] = cols if gain is None else gain * cols
        out_ref[peer] = row[...].astype(BF16)


def packed(layers):
    gains = [layer[0][None, :] for layer in layers]
    matrices = [matrix for layer in layers for matrix in layer[1:]]
    vmem = pl.BlockSpec(memory_space=pltpu.VMEM)
    width = len(matrices) * PART
    return pl.pallas_call(
        pack_kernel,
        out_shape=jax.ShapeDtypeStruct((Y * X, ROWS, width), BF16),
        in_specs=[vmem] * len(gains) + [pl.BlockSpec(memory_space=pl.ANY)] * len(matrices),
        out_specs=vmem,
        scratch_shapes=[
            pltpu.VMEM((len(matrices), *matrices[0].shape), F32),
            pltpu.VMEM((BUFFERS, ROWS, width), F32),
            pltpu.SemaphoreType.DMA((len(matrices),)),
        ],
        cost_estimate=pl.CostEstimate(flops=10**6, bytes_accessed=10**6, transcendentals=0),
        name="pack",
    )(*gains, *matrices)


def by_block(to_yx):
    here = swap(to_yx, ("y", "x")).reshape(Y, X, ROWS, -1)
    turned = here.transpose(1, 3, 0, 2).reshape(X, -1, PART, LANES)
    return jnp.pad(turned, ((0, 0), (0, 0), (0, PADDED - PART), (0, 0))).reshape(X, -1, LANES)


def by_span(parts):
    to_z = jnp.broadcast_to(parts[None], (GR, *parts.shape)).reshape(GR * ZQ, *parts.shape[1:])
    here = swap(to_z, ("gr", "zq"))
    return [here[:, i : i + PIECE] for i in range(0, here.shape[1], PIECE)]


def paired(piece):
    near = from_peer(piece, "b", B, 1)
    low = lax.axis_index("b") == 0
    both = jnp.stack([jnp.where(low, piece, near), jnp.where(low, near, piece)], axis=1)
    return both.reshape(SPANS, PIECE, LANES)


def over_x(pair):
    one, three = (from_peer(pair, "x", X, k) for k in (1, 3))
    two = from_peer(pair, "x", X, 2)
    return [pair, one, two, three]


def over_core(pieces):
    own, one, three = (from_peer(pieces[k], "core", CORE, 1) for k in (0, 1, 3))
    two = from_peer(pieces[2], "core", CORE, 1)
    return [own, one, two, three]


def slot(zl, zq):
    k = (zl // B) ^ zq
    return ((k & 1) << 1) | (k >> 1), zl % B


def half_kernel(at_ref, x_ref, *refs):
    piece_refs, (out_ref, acc_ref, sq_ref) = refs[: 2 * X], refs[2 * X :]
    width = x_ref.shape[-1]
    pieces = 2 * X
    zq = at_ref[0]

    def rows(span, lo, hi):
        return jnp.concatenate([ref[span, lo:hi, :] for ref in piece_refs], axis=0)

    def both(zl, lo, hi):
        return jnp.concatenate([rows(2 * zl, lo, hi), rows(2 * zl + 1, lo, hi)], axis=1)

    acc_ref[...] = jnp.zeros_like(acc_ref)
    sq_ref[...] = jnp.zeros_like(sq_ref)

    def inward(z, _):
        k, _ = slot(z * B, zq)
        tokens = jnp.concatenate([x_ref[:, k, b].reshape(Y * FEATS, width) for b in range(B)], axis=0)
        wide = tokens.astype(F32)
        sq_ref[...] += jnp.sum((wide * wide).reshape(B * Y * FEATS // 8, 8, width), axis=0)
        weights = jnp.concatenate([both(z * B + b, 0, 2 * PADDED) for b in range(B)], axis=1)
        acc_ref[...] += jnp.dot(weights, tokens, preferred_element_type=F32)
        return 0

    lax.fori_loop(0, ZQ, inward, 0)
    squares = jnp.sum(sq_ref[...], axis=0, keepdims=True)
    scale = lax.rsqrt(squares / D + NORM_EPS) * D ** (-0.5)
    sums = acc_ref[...].reshape(pieces, 2 * PADDED, width)
    gate = sums[:, :PADDED].reshape(pieces * PADDED, width) * scale
    up = sums[:, PADDED:].reshape(pieces * PADDED, width) * scale
    hidden = (gate / (1.0 + jnp.exp(-gate)) * up).astype(BF16)

    def outward(zl, _):
        part = lax.dot_general(
            both(zl, 2 * PADDED, PIECE), hidden, (((0,), (0,)), ((), ())), preferred_element_type=F32
        )
        k, b = slot(zl, zq)
        out_ref[:, k, b] = part.astype(BF16).reshape(Y, FEATS, width)
        return 0

    lax.fori_loop(0, ZL, outward, 0)


def half_partial(tokens, pieces):
    width = tokens.shape[-1]
    vmem = pl.BlockSpec(memory_space=pltpu.VMEM)
    flops = 2 * 3 * 2 * X * PADDED * D * width
    return pl.pallas_call(
        half_kernel,
        out_shape=jax.ShapeDtypeStruct(tokens.shape, BF16),
        in_specs=[pl.BlockSpec(memory_space=pltpu.SMEM)] + [vmem] * (1 + 2 * X),
        out_specs=vmem,
        scratch_shapes=[pltpu.VMEM((2 * X * 2 * PADDED, width), F32), pltpu.VMEM((8, width), F32)],
        cost_estimate=pl.CostEstimate(
            flops=flops, bytes_accessed=2 * (2 * tokens.size + 2 * X * pieces[0].size), transcendentals=0
        ),
        compiler_params=pltpu.CompilerParams(vmem_limit_bytes=20 * MIB),
        name="half_step",
    )(place("zq"), tokens, *pieces)


def serve_kernel(at_ref, *refs):
    piece_refs, out_refs, rows_ref = refs[: 2 * X], refs[2 * X : -1], refs[-1]
    x, here = at_ref[0], at_ref[1] == at_ref[2]
    odd, high = (x & 1) == 1, (x & 2) == 2
    for span in range(AT_ONCE):
        for m, out_ref in enumerate(out_refs):
            lo, hi = m * PADDED, (m + 1) * PADDED
            mine = [ref[span, lo:hi, :].astype(F32) for ref in piece_refs[:X]]
            other = [ref[span, lo:hi, :].astype(F32) for ref in piece_refs[X:]]
            p = [jnp.where(here, a, b) for a, b in zip(mine, other)]
            p = [jnp.where(odd, p[k ^ 1], p[k]) for k in range(X)]
            p = [jnp.where(high, p[k ^ 2], p[k]) for k in range(X)]
            for k in range(X):
                rows_ref[m, k * PART : (k + 1) * PART, :] = p[k][:PART]
            out_ref[:, span * LANES : (span + 1) * LANES] = rows_ref[m].astype(BF16)


def served(pieces):
    piece = pl.BlockSpec((AT_ONCE, PIECE, LANES), lambda j, at: (j, 0, 0))
    out = pl.BlockSpec((BLOCK, AT_ONCE * LANES), lambda j, at: (0, j))
    return pl.pallas_call(
        serve_kernel,
        out_shape=[jax.ShapeDtypeStruct((BLOCK, D), BF16)] * 3,
        grid_spec=pltpu.PrefetchScalarGridSpec(
            num_scalar_prefetch=1,
            grid=(SPANS // AT_ONCE,),
            in_specs=[piece] * (2 * X),
            out_specs=[out] * 3,
            scratch_shapes=[pltpu.VMEM((3, BLOCK, LANES), F32)],
        ),
        cost_estimate=pl.CostEstimate(
            flops=10**8, bytes_accessed=2 * (2 * X * pieces[0].size + 3 * BLOCK * D), transcendentals=0
        ),
        compiler_params=pltpu.CompilerParams(vmem_limit_bytes=16 * MIB),
        name="serve",
    )(place("x", "core", "b"), *pieces)


def place(*axes):
    return jnp.stack([lax.axis_index(axis) for axis in axes]).astype(jnp.int32)


def traded(first, second):
    low = lax.axis_index("b") == 0
    keep, send = jnp.where(low, first, second), jnp.where(low, second, first)
    got = from_peer(send, "b", B, 1)
    return jnp.where(low, keep, got), jnp.where(low, got, keep)


def far_zq(tokens):
    return jnp.stack([tokens, from_peer(tokens, "zq", ZQ, 2)])


def near_zq(two):
    return jnp.concatenate([two, from_peer(two, "zq", ZQ, 1)])


def kept_half(by_y):
    send = jnp.sum(by_y[:, ZQ // 2 :].astype(F32), axis=0).astype(BF16)
    got = from_peer(send, "zq", ZQ, 1)
    return jnp.sum(by_y[:, : ZQ // 2].astype(F32), axis=0) + got.astype(F32)


def summed_twice(by_y):
    kept = kept_half(by_y).astype(BF16)
    got = from_peer(kept, "zq", ZQ, 2)
    return kept.astype(F32) + got[::-1].astype(F32)


def brought_home(by_y):
    near, far = kept_half(by_y).astype(BF16)
    low = lax.axis_index("b") == 0

    def own(block):
        return jnp.where(low, block[0], block[1])

    def peer(block):
        return jnp.where(low, block[1], block[0])

    here = own(near).astype(F32) + from_peer(own(far), ("zq", "b"), ZL, 4).astype(F32)
    there = from_peer(peer(near), ("zq", "b"), ZL, 1).astype(F32)
    there += from_peer(peer(far), ("zq", "b"), ZL, 5).astype(F32)
    return jnp.where(low, here, there), jnp.where(low, there, here)


def stepped(tokens, total):
    return (tokens.astype(F32) + 0.5 * FF ** (-0.5) * total).astype(BF16)


def local(prompt, gain_pre, gate_pre, up_pre, down_pre, gain_post, gate_post, up_post, down_post):
    half = prompt.shape[0] // B
    turned = prompt.T
    parts = by_block(
        packed([(gain_pre, gate_pre, up_pre, down_pre), (gain_post, gate_post, up_post, down_post)])
    )
    tokens = jnp.stack(traded(turned[:, :half], turned[:, half:]))
    parts, two_away = lax.optimization_barrier((parts, far_zq(tokens)))
    one, two = by_span(parts)
    wide = after(two_away, one)
    one = paired(one)
    wide = near_zq(wide)
    pieces = over_x(one)
    wide = share(wide, "y", Y)
    two = paired(after(two, one))
    pieces += over_core(pieces)
    wide, two, *pieces = lax.optimization_barrier((wide, two, *pieces))
    partial = half_partial(wide, pieces)
    partial, two, *pieces = lax.optimization_barrier((partial, two, *pieces))
    first = served(pieces)
    pieces = over_x(two)
    by_y = swap(partial, "y")
    total, *first = lax.optimization_barrier((summed_twice(by_y), *first))
    total, *pieces = lax.optimization_barrier((total, *pieces))
    middle = stepped(two_away, total)
    pieces += over_core(pieces)

    partial = half_partial(share(near_zq(middle), "y", Y), pieces)
    base = traded(middle[0, 0], middle[0, 1])
    partial, base, *pieces = lax.optimization_barrier((partial, base, *pieces))
    second = served(pieces)
    by_y, *second = lax.optimization_barrier((swap(partial, "y"), *second))
    back = jnp.concatenate([stepped(*half) for half in zip(base, brought_home(by_y))], axis=1)
    return (back.T, *first, *second)


def solution(mesh):
    fine = Mesh(mesh.devices.reshape(GR, ZQ, B, Y, X, CORE), AXES)
    tokens = P(("gr", "x", "core"), ("zq", "b", "y"))
    gain = P(("gr", "zq", "b", "y"))
    trained = P(("gr", "zq", "b", "y"), ("x", "core"))
    rows = P(("zq", "b", "y"), None)
    return jax.shard_map(
        local,
        mesh=fine,
        in_specs=(tokens, gain, trained, trained, trained, gain, trained, trained, trained),
        out_specs=(tokens,) + (rows,) * 6,
        check_vma=False,
    )
```
